32 devices in a mesh: ep: 16 (over z, x, core), tp: 2 (over y).
Axes of the slice: x: 2, y: 2, z: 4, core: 2. Of those that a mesh axis runs over, the one named last changes fastest.
Arguments:
- tokens: bfloat16 [192, 4096], P('ep', 'tp')
- norm_gain: float32 [4096], P('tp'), may hold values from 0.1 to 1.9
- routes: int32 [192, 6], P('ep'), may hold values from 0 to 15, all different within a row; in each aligned block of 12 rows (0 to 11, 12 to 23, ...) at most 5 rows name the same one
- route_weights: float32 [192, 6], P('ep'), may hold values from 0.05 to 1
- expert_gate: bfloat16 [16, 4096, 1024], P('ep', 'tp'), may hold values from -0.09375 to 0.09375
- expert_up: bfloat16 [16, 4096, 1024], P('ep', 'tp'), may hold values from -0.09375 to 0.09375
- expert_down: bfloat16 [16, 1024, 4096], P('ep', None, 'tp'), may hold values from -0.1875 to 0.1875
- shared_gate: bfloat16 [4096, 1024], P('tp'), may hold values from -0.09375 to 0.09375
- shared_up: bfloat16 [4096, 1024], P('tp'), may hold values from -0.09375 to 0.09375
- shared_down: bfloat16 [1024, 4096], P(None, 'tp'), may hold values from -0.1875 to 0.1875
Outputs:
- mixed: bfloat16 [192, 4096], P('ep', 'tp')
The draws below stay inside these ranges and needn't reach their ends.
Inputs may be any that keep to these rules, and one draw needn't show every extreme that they name: `routes`: each row names 6 different experts; among the rows of one device no expert is named more than 5 times, and in some devices' rows one expert is named exactly 5 times.
All inputs are finite; a program needn't handle non-finite values.
Results may differ from the reference program's by a relative error of at most 0.0068.
Values may be sent and summed in bfloat16 or wider, within the bound.
A program may use at most 64 MiB of HBM per device.

```python
import math
import jax
import jax.numpy as jnp
import numpy as np
from jax import lax

D = 4096
FF_E = 1024
FF_S = 1024
TOP_K = 6
TOK_DEV = 12
EXPERTS = 16
CAP = 5
TOKENS = 192
N_EP = 16


def draw_tokens(key, part):
    first, second = jax.random.split(jax.random.fold_in(key, 11), 2)
    column = jnp.arange(D, dtype=jnp.float32) / D
    rising = jnp.exp(jnp.log(8.0) * column)[None, :]
    base = jax.random.normal(first, (TOKENS, D), jnp.float32)
    rough = jax.random.uniform(second, (1, D), jnp.float32, 0.5, 1.5)
    values = jnp.clip(base, -6.0, 6.0) * rough * rising
    return values.astype(jnp.bfloat16)


def block_levels(key, shape, cuts, least, high):
    def one(dim, parts):
        steps = jax.random.uniform(jax.random.fold_in(jax.random.fold_in(key, 6), dim), (parts,), jnp.float32, least / len(cuts), high / len(cuts))
        return jnp.repeat(jnp.exp(steps), shape[dim] // parts).reshape((-1,) + (1,) * (len(shape) - dim - 1))

    level = one(*cuts[0])
    for cut in cuts[1:]:
        level = level * one(*cut)
    return level


def deal_out(stream_key, own, number, rows, count, top, limit, lean):
    sequence = jax.random.permutation(stream_key, count)
    heavy_load, common = shares(count, rows * top, limit, lean, True), shares(count, rows * top, limit, lean, False)
    places = jnp.arange(count)

    def named(tallies, offset_by):
        used = int((tallies > 0).sum())
        fixed = max(1, used // 4)
        moved = fixed + (places - fixed + offset_by * (used - fixed)) % max(1, count - fixed)
        return jnp.zeros((count,), jnp.int32).at[sequence[jnp.where(places < fixed, places, moved)]].set(jnp.asarray(tallies, jnp.int32))

    tallies = jnp.where(number % 4 == 0, named(heavy_load, number // 4), named(common, number - number // 4 - 1))
    mixed = jax.random.permutation(jax.random.fold_in(own, 3), count)
    donor, receiver = mixed[0:count // 2 * 2:2], mixed[1:count // 2 * 2:2]
    room = jnp.minimum(tallies[donor] - 1, limit - tallies[receiver]) // 2
    room = jnp.where((donor == sequence[0]) | (receiver == sequence[0]) | (tallies[receiver] == 0), 0, jnp.maximum(room, 0))
    moved = jax.random.randint(jax.random.fold_in(own, 4), (count // 2,), 0, 1 << 20) % (room + 1)
    tallies = tallies.at[donor].add(-moved).at[receiver].add(moved)
    labels = jnp.searchsorted(jnp.cumsum(tallies), jnp.arange(rows * top), side="right").astype(jnp.int32)
    grid = labels.reshape(top, rows).T
    grid = grid[jax.random.permutation(jax.random.fold_in(own, 1), rows)]
    offset_by = jax.random.randint(jax.random.fold_in(own, 2), (rows, 1), 0, top)
    return jnp.take_along_axis(grid, (jnp.arange(top)[None, :] + offset_by) % top, axis=1)


def shares(count, total, most, slope, full):
    weights = [(1 << 20) // math.isqrt(rank ** slope) + 1 for rank in range(1, count + 1)]
    largest = most if full else min(most, max(-(-total // count), total * weights[0] // sum(weights)))
    least = 1 if total - largest >= count - 1 else 0
    given, spare = [largest] + [least] * (count - 1), total - largest - least * (count - 1)
    while spare > 0:
        free = [i for i in range(1, count) if given[i] < largest] or [i for i in range(1, count) if given[i] < most]
        whole, budget = sum([weights[i] for i in free]), spare
        for i in free:
            addition = min(most - given[i], max(1, budget * weights[i] // whole), spare)
            given[i] = given[i] + addition
            spare = spare - addition
    return np.array(given)


def normal_values(own_key, dims, width, bound, cuts=(), held_as=jnp.bfloat16):
    entries = jax.random.normal(own_key, dims, jnp.float32) * width
    if len(cuts) > 0:
        entries = block_levels(own_key, dims, cuts, -0.22, 0.18) * entries
    return jnp.clip(entries, min=-bound, max=bound).astype(held_as)


def setup_inputs(seed: int = 0) -> dict:
    streams_of = jax.random.split(jax.random.key(seed), 11)
    tokens = draw_tokens(jax.random.fold_in(streams_of[10], 71), 0)
    norm_gain = jnp.clip(1.0 + 0.18 * jax.random.normal(streams_of[1], (D,), jnp.float32), 0.1, 1.9)
    routes_keys = jax.random.split(jax.random.fold_in(streams_of[2], 1), TOKENS // TOK_DEV)
    routes_turns = jax.random.permutation(jax.random.fold_in(streams_of[2], 3), TOKENS // TOK_DEV)
    routes = jax.vmap(lambda own, number: deal_out(jax.random.fold_in(streams_of[2], 2), own, number, TOK_DEV, EXPERTS, TOP_K, CAP, 2))(routes_keys, routes_turns).reshape((TOKENS, TOP_K))
    route_weights = jnp.clip(jnp.exp(math.log(1.0) - 2.9957323 * jax.random.uniform(streams_of[3], (TOKENS, TOP_K), jnp.float32) ** block_levels(streams_of[3], (TOKENS, TOP_K), ((0, 16),), -0.2, 0.2)), 0.05, 1.0)
    expert_gate = normal_values(streams_of[4], (EXPERTS, D, FF_E), D ** -0.5, 0.09375, ((0, 16), (1, 2)))
    expert_up = normal_values(streams_of[5], (EXPERTS, D, FF_E), D ** -0.5, 0.09375, ((0, 16), (1, 2)))
    expert_down = normal_values(streams_of[6], (EXPERTS, FF_E, D), FF_E ** -0.5, 0.1875, ((0, 16), (2, 2)))
    shared_gate = normal_values(streams_of[7], (D, FF_S), D ** -0.5, 0.09375, ((0, 2),))
    shared_up = normal_values(streams_of[8], (D, FF_S), D ** -0.5, 0.09375, ((0, 2),))
    shared_down = normal_values(streams_of[9], (FF_S, D), FF_S ** -0.5, 0.1875, ((1, 2),))
    return {"tokens": tokens, "norm_gain": norm_gain, "routes": routes, "route_weights": route_weights, "expert_gate": expert_gate, "expert_up": expert_up, "expert_down": expert_down, "shared_gate": shared_gate, "shared_up": shared_up, "shared_down": shared_down}


def block_ranks(route_blocks, n_experts):
    onehot = (route_blocks[..., None] == jnp.arange(n_experts, dtype=jnp.int32)).astype(jnp.int32)
    before = jnp.cumsum(onehot, axis=1) - onehot
    return lax.optimization_barrier(jnp.sum(before * onehot, axis=-1))

def expert_tables(route_blocks, weight_blocks, expert, capacity, n_experts):
    blocks, tok, picks = route_blocks.shape
    ranks = block_ranks(route_blocks.reshape(blocks, tok * picks), n_experts).reshape(blocks, tok, picks)
    slot = jnp.where(route_blocks == expert, ranks, -1)
    hits = slot[..., None] == jnp.arange(capacity, dtype=jnp.int32)
    select = jnp.any(hits, axis=2).astype(jnp.float32)
    weighted = lax.optimization_barrier(jnp.sum(jnp.where(hits, weight_blocks[..., None], 0.0), axis=2))
    return (select, weighted)

def swiglu(rows, gate_w, up_w, down_w):
    gate = jnp.dot(rows, gate_w, preferred_element_type=jnp.float32)
    up = jnp.dot(rows, up_w, preferred_element_type=jnp.float32)
    hidden = (jax.nn.silu(gate) * up).astype(jnp.bfloat16)
    return jnp.dot(hidden, down_w, preferred_element_type=jnp.float32)

def reference(tokens, norm_gain, routes, route_weights, expert_gate, expert_up, expert_down, shared_gate, shared_up, shared_down):
    values = tokens.astype(jnp.float32)
    meansq = lax.optimization_barrier(jnp.mean(values * values, axis=1, keepdims=True))
    normed = (values * lax.rsqrt(meansq + 1e-06) * norm_gain.astype(jnp.float32)[None, :]).astype(jnp.bfloat16)
    scaled = 2.5 * route_weights / lax.optimization_barrier(jnp.sum(route_weights, axis=1, keepdims=True))
    shared_out = swiglu(normed, shared_gate, shared_up, shared_down)
    capacity = max(2, TOK_DEV * TOP_K // N_EP + 1)
    route_blocks = routes.reshape(N_EP, TOK_DEV, TOP_K)
    weight_blocks = scaled.reshape(N_EP, TOK_DEV, TOP_K)
    x_blocks = normed.reshape(N_EP, TOK_DEV, D).astype(jnp.float32)

    def one_expert(carry, packed):
        gate_w, up_w, down_w, expert = packed
        select, weighted = expert_tables(route_blocks, weight_blocks, expert, capacity, EXPERTS)
        rows = jnp.einsum('stc,std->scd', select, x_blocks).astype(jnp.bfloat16)
        result = swiglu(rows.reshape(N_EP * capacity, D), gate_w, up_w, down_w).astype(jnp.bfloat16)
        result = result.reshape(N_EP, capacity, D).astype(jnp.float32)
        carry = carry + jnp.einsum('stc,scd->std', weighted, result, precision=lax.Precision.HIGHEST)
        return (carry, None)
    start = jnp.zeros((N_EP, TOK_DEV, D), jnp.float32)
    routed, _ = lax.scan(one_expert, start, (expert_gate, expert_up, expert_down, jnp.arange(EXPERTS, dtype=jnp.int32)))
    return (shared_out + routed.reshape(TOKENS, D)).astype(jnp.bfloat16)
```

```python
import functools

import jax
import jax.numpy as jnp
from jax import lax
from jax.experimental import pallas as pl
from jax.experimental.pallas import tpu as pltpu
from jax.sharding import PartitionSpec as P

MESH = pl.DeviceIdType.MESH
F32 = jnp.float32
BF16 = jnp.bfloat16
LANES = 128
TN = (((0,), (0,)), ((), ()))


def silu_mul(g, u):
    return g / (1.0 + jnp.exp(-g)) * u


def kernel(
    n, tp, cap, chunks, pieces,
    x_hbm, gain_hbm, routes_hbm, rw_hbm,
    eg_hbm, eu_hbm, ed_hbm, sg_hbm, su_hbm, sd_hbm,
    out_ref,
    wg, wu, wd, vg, vu, vd,
    x_ref, gain_ref, routes_ref, rw_ref, xm_ref, meta, metam,
    packed, outbuf, arrive, retbuf, back,
    rows, sssend, ssrecv, shsend, shrecv, acc, shout,
    isem, wsem, dsend, drecv, rsend, rrecv, tsend, trecv, qsend, qrecv, hsend, hrecv, xsend, xrecv,
    *exchanged,
):
    me = lax.axis_index("ep")
    my_tp = lax.axis_index("tp")
    m, quarter = n // 2, n // 4
    half, inner = me // m, lax.rem(me, m)
    mirror = lax.rem(me + m, n)
    spot = lax.rem(me, quarter)
    toks, width = x_ref.shape
    picks = routes_ref.shape[0]
    ff = wg.shape[1]
    fs = vg.shape[1]
    blocks = width // LANES
    jc = blocks * cap
    cols = ff // chunks
    mine, psend, precv = exchanged[0::3], exchanged[1::3], exchanged[2::3]

    def mate(i):
        return half * m + lax.rem(inner + i, m)

    def in_quarter(q):
        return [q * quarter + lax.rem(spot + i, quarter) for i in range(quarter)]

    near = [mate(i) for i in range(m)]
    groups = [near, in_quarter(2 * (1 - half)), in_quarter(2 * (1 - half) + 1)]

    barrier = pltpu.get_barrier_semaphore()
    pl.semaphore_signal(barrier, inc=1, device_id={"ep": mirror}, device_id_type=MESH)
    for i in range(1, m):
        pl.semaphore_signal(barrier, inc=1, device_id={"ep": mate(i)}, device_id_type=MESH)
    for i in range(1, tp):
        pl.semaphore_signal(barrier, inc=1, device_id={"tp": lax.rem(my_tp + i, tp)}, device_id_type=MESH)

    small = []
    for i, (src, dst) in enumerate(
        ((routes_hbm, routes_ref), (rw_hbm, rw_ref), (x_hbm, x_ref), (gain_hbm, gain_ref))
    ):
        c = pltpu.make_async_copy(src, dst, isem.at[i])
        c.start()
        small.append(c)
    for c in small:
        c.wait()
    loads = {}
    slot = 0
    for name, src, dst in (
        ("eg", eg_hbm.at[0], wg), ("eu", eu_hbm.at[0], wu), ("sg", sg_hbm, vg), ("su", su_hbm, vu),
        ("ed", ed_hbm.at[0], wd), ("sd", sd_hbm, vd),
    ):
        depth = dst.shape[0] // pieces
        loads[name] = []
        for i in range(pieces):
            c = pltpu.make_async_copy(
                src.at[pl.ds(i * depth, depth)], dst.at[pl.ds(i * depth, depth)], wsem.at[slot]
            )
            c.start()
            loads[name].append(c)
            slot += 1

    def loaded(*names):
        for name in names:
            for c in loads[name]:
                c.wait()

    def places(routes, base, number):
        expert = lax.broadcasted_iota(jnp.int32, (number, toks), 0) + base
        hits = [routes[k : k + 1, :] == expert for k in range(picks)]
        named = jnp.zeros((number, toks), F32)
        for hit in hits:
            named = named + jnp.where(hit, 1.0, 0.0)
        row_i = lax.broadcasted_iota(jnp.int32, (toks, toks), 0)
        col_i = lax.broadcasted_iota(jnp.int32, (toks, toks), 1)
        earlier = jnp.where(row_i < col_i, 1.0, 0.0).astype(BF16)
        before = jnp.dot(named.astype(BF16), earlier, preferred_element_type=F32)
        return hits, jnp.where(named > 0.5, before, -1.0)

    def by_slot(place, v):
        return jnp.concatenate([jnp.where(place == s, v, 0.0) for s in range(cap)], axis=0).astype(BF16)

    def pack(value, j, number):
        for s in range(cap):
            packed[pl.ds(j * cap + s, number, stride=jc), :] = value[s * number : (s + 1) * number, :]

    def unpack(j, number):
        return jnp.concatenate(
            [packed[pl.ds(j * cap + s, number, stride=jc), :] for s in range(cap)], axis=0
        )

    def select_rows(g, routes, x):
        select = by_slot(places(routes, half * m, m)[1], 1.0)
        for j in range(blocks):
            cut = slice(j * LANES, (j + 1) * LANES)
            pack(jnp.dot(select, x[:, cut], preferred_element_type=F32), j, m)
        for p in range(m):
            outbuf[g, p] = packed[pl.ds(p * jc, jc), :].astype(BF16)

    pending = []

    def to_tp(src, dst_of, send_of, recv_of):
        copies = []
        for i in range(1, tp):
            c = pltpu.make_async_remote_copy(
                src_ref=src, dst_ref=dst_of(i - 1), send_sem=send_of(i - 1), recv_sem=recv_of(i - 1),
                device_id={"tp": lax.rem(my_tp + i, tp)}, device_id_type=MESH,
            )
            c.start()
            copies.append(c)
        pending.extend(copies)
        return copies

    def to_mirror(src, dst, at):
        c = pltpu.make_async_remote_copy(
            src_ref=src, dst_ref=dst, send_sem=xsend.at[at], recv_sem=xrecv.at[at],
            device_id={"ep": mirror}, device_id_type=MESH,
        )
        c.start()
        pending.append(c)
        return c

    def send_tokens(g, home):
        for i in range(1, m):
            to = lax.rem(inner + i, m)
            c = pltpu.make_async_remote_copy(
                src_ref=outbuf.at[g, to], dst_ref=arrive.at[home], send_sem=dsend.at[g, to], recv_sem=drecv.at[home],
                device_id={"ep": mate(i)}, device_id_type=MESH,
            )
            c.start()
            pending.append(c)
        arrive[home] = outbuf[g, inner]

    def wait_tokens(g):
        for i, home in enumerate(groups[g]):
            if g == 0 and i == 0:
                continue
            copy = pltpu.make_async_remote_copy(
                src_ref=outbuf.at[0, 0], dst_ref=arrive.at[home], send_sem=dsend.at[0, 0], recv_sem=drecv.at[home],
                device_id={"ep": mate(1)}, device_id_type=MESH,
            )
            if g == 0:
                copy.wait_recv()
            else:
                @pl.when(home != mirror)
                def _(copy=copy):
                    copy.wait_recv()

    def send_back(g):
        for i, home in enumerate(groups[g]):
            if g or i:
                c = pltpu.make_async_remote_copy(
                    src_ref=retbuf.at[home], dst_ref=back.at[me], send_sem=rsend.at[home], recv_sem=rrecv.at[me],
                    device_id={"ep": home}, device_id_type=MESH,
                )
                c.start()
                pending.append(c)

    def wait_back(g):
        for i, frm in enumerate(groups[g]):
            if g or i:
                pltpu.make_async_remote_copy(
                    src_ref=retbuf.at[frm], dst_ref=back.at[frm], send_sem=rsend.at[frm], recv_sem=rrecv.at[frm],
                    device_id={"ep": frm}, device_id_type=MESH,
                ).wait_recv()

    routes = routes_ref[...]
    meta[0:picks, 0:toks] = routes.astype(F32)
    x = x_ref[...]
    gain = gain_ref[...]
    select_rows(0, routes, x)
    pl.semaphore_wait(barrier, m + tp - 1)
    mcopy = to_mirror(meta, metam, 1)
    xcopy = to_mirror(x_ref, xm_ref, 0)
    send_tokens(0, me)
    rw = rw_ref[...]
    scaled = 2.5 * rw / jnp.sum(rw, axis=0, keepdims=True)
    hits, place = places(routes, 0, n)
    weight = jnp.zeros((n, toks), F32)
    for k in range(picks):
        weight = weight + jnp.where(hits[k], scaled[k : k + 1, :], 0.0)
    w_hi = weight.astype(BF16).astype(F32)
    comb_hi, comb_lo = by_slot(place, w_hi), by_slot(place, weight - w_hi)
    rows[...] = jnp.zeros(rows.shape, BF16)
    mcopy.wait_recv()
    routes_m = metam[0:picks, 0:toks].astype(jnp.int32)
    xcopy.wait_recv()
    select_rows(1, routes_m, xm_ref[...])
    send_tokens(1, mirror)

    def start_shared():
        xf = x.astype(F32)
        xg = (xf * gain).astype(BF16)
        ss_own = jnp.sum(xf * xf, axis=1, keepdims=True)
        shsend[...] = jnp.zeros(shsend.shape, F32)
        shsend[0:toks, 2 * fs : 2 * fs + LANES] = jnp.broadcast_to(ss_own, (toks, LANES))
        for name, w, base in (("sg", vg, 0), ("su", vu, fs)):
            loaded(name)
            shsend[0:toks, base : base + fs] = jnp.dot(xg, w[...], preferred_element_type=F32)

    def send_shared():
        return to_tp(shsend, lambda i: shrecv.at[i], lambda i: hsend.at[i], lambda i: hrecv.at[i])

    def finish_shared(copies):
        loaded("sd")
        for c in copies:
            c.wait_recv()
        total = shsend[...]
        for i in range(tp - 1):
            total = total + shrecv[i]
        r_own = lax.rsqrt(total[:, 2 * fs : 2 * fs + 1] / (width * tp) + 1e-06)
        sh_hidden = silu_mul(total[:, 0:fs] * r_own, total[:, fs : 2 * fs] * r_own).astype(BF16)
        shout[...] = jnp.dot(sh_hidden, vd[...], preferred_element_type=F32)

    starts = []
    for g in range(len(groups)):
        starts.append(sum(-(-len(groups[i]) * cap // 8) * 8 for i in range(g)))

    def first_half(g):
        number = len(groups[g])
        count, base = number * cap, starts[g]
        low = -(-count // 16) * 16
        wait_tokens(g)
        for i, home in enumerate(groups[g]):
            packed[pl.ds(i * jc, jc), :] = arrive[home].astype(F32)
        ss = jnp.zeros((count, LANES), F32)
        for j in range(blocks):
            cut = slice(j * LANES, (j + 1) * LANES)
            piece = unpack(j, number)
            ss = ss + piece * piece
            scaled_piece = piece * gain[:, cut]
            hi = scaled_piece.astype(BF16)
            rows[0:count, cut] = hi
            rows[low : low + count, cut] = (scaled_piece - hi.astype(F32)).astype(BF16)
        sssend[base : base + count] = jnp.broadcast_to(jnp.sum(ss, axis=1, keepdims=True), (count, LANES))
        part = pl.ds(base, count)
        all_copies = [to_tp(
            sssend.at[part], lambda i: ssrecv.at[i, part],
            lambda i: qsend.at[i * len(groups) + g], lambda i: qrecv.at[i * len(groups) + g],
        )]
        taken_rows = rows[0 : 2 * low, :]
        for c in range(chunks):
            cut = slice(c * cols, (c + 1) * cols)
            for w, at in ((wg, 0), (wu, cols)):
                v = jnp.dot(taken_rows, w[:, cut], preferred_element_type=F32)
                v = v[0:count] + v[low : low + count]
                mine[g][c, :, at : at + cols] = v
                psend[g][c, :, at : at + cols] = v.astype(BF16)
            at_sem = lambda i: (i * len(groups) + g) * chunks + c
            all_copies.append(to_tp(
                psend[g].at[c], lambda i: precv[g].at[i, c],
                lambda i: tsend.at[at_sem(i)], lambda i: trecv.at[at_sem(i)],
            ))
        return all_copies

    def second_half(g, all_copies):
        number = len(groups[g])
        count, base = number * cap, starts[g]
        for c in all_copies[0]:
            c.wait_recv()
        ss_all = sssend[base : base + count, :]
        for i in range(tp - 1):
            ss_all = ss_all + ssrecv[i, base : base + count, :]
        r = lax.rsqrt(ss_all[:, 0:1] / (width * tp) + 1e-06)
        for c in range(chunks):
            for copy in all_copies[1 + c]:
                copy.wait_recv()
            both = mine[g][c]
            for i in range(tp - 1):
                both = both + precv[g][i, c].astype(F32)
            hidden = silu_mul(both[:, 0:cols] * r, both[:, cols : 2 * cols] * r).astype(BF16)
            part = jnp.dot(hidden, wd[c * cols : (c + 1) * cols, :], preferred_element_type=F32)
            if c == 0:
                acc[0:count, :] = part
            elif c < chunks - 1:
                acc[0:count, :] += part
            else:
                for j in range(blocks):
                    cut = slice(j * LANES, (j + 1) * LANES)
                    pack(acc[0:count, cut] + part[:, cut], j, number)
        for i, home in enumerate(groups[g]):
            retbuf[home] = packed[pl.ds(i * jc, jc), :].astype(BF16)
        send_back(g)

    loaded("eg", "eu")
    state0 = first_half(0)
    start_shared()
    state1 = first_half(1)
    state2 = first_half(2)
    shared = send_shared()
    loaded("ed")
    second_half(0, state0)
    back[me] = retbuf[me]
    second_half(1, state1)
    second_half(2, state2)
    finish_shared(shared)
    for g in range(len(groups)):
        wait_back(g)
    for p in range(n):
        packed[pl.ds(p * jc, jc), :] = back[p].astype(F32)
    for j in range(blocks):
        cut = slice(j * LANES, (j + 1) * LANES)
        piece = unpack(j, n).astype(BF16)
        routed = lax.dot_general(comb_hi, piece, TN, preferred_element_type=F32)
        routed = routed + lax.dot_general(comb_lo, piece, TN, preferred_element_type=F32)
        out_ref[:, cut] = (shout[0:toks, cut] + routed).astype(BF16)
    for c in pending:
        c.wait_send()


def local(tokens, norm_gain, routes, route_weights, eg, eu, ed, sg, su, sd):
    toks, width = tokens.shape
    picks = routes.shape[1]
    n, tp = lax.axis_size("ep"), lax.axis_size("tp")
    cap = max(2, toks * picks // n + 1)
    ff, fs = eg.shape[2], sg.shape[1]
    chunks, pieces = 2, 4
    m, quarter = n // 2, n // 4
    jc = width // LANES * cap
    low = -(-m * cap // 16) * 16
    padded = -(-toks // 16) * 16
    cols = ff // chunks
    others = max(1, tp - 1)
    split = -(-picks // 8) * 8
    sizes = (m, quarter, quarter)
    total_rows = sum(-(-s * cap // 8) * 8 for s in sizes)
    exchanged = []
    for s in sizes:
        exchanged += [
            pltpu.VMEM((chunks, s * cap, 2 * cols), F32),
            pltpu.VMEM((chunks, s * cap, 2 * cols), BF16),
            pltpu.VMEM((others, chunks, s * cap, 2 * cols), BF16),
        ]
    hbm = pl.BlockSpec(memory_space=pl.ANY)
    dma = pltpu.SemaphoreType.DMA
    return pl.pallas_call(
        functools.partial(kernel, n, tp, cap, chunks, pieces),
        out_shape=pltpu.VMEM((toks, width), BF16),
        in_specs=[hbm] * 10,
        out_specs=pl.BlockSpec(memory_space=pltpu.VMEM),
        scratch_shapes=[
            pltpu.VMEM((width, ff), BF16), pltpu.VMEM((width, ff), BF16), pltpu.VMEM((ff, width), BF16),
            pltpu.VMEM((width, fs), BF16), pltpu.VMEM((width, fs), BF16), pltpu.VMEM((fs, width), BF16),
            pltpu.VMEM((toks, width), BF16), pltpu.VMEM((1, width), F32),
            pltpu.VMEM((picks, toks), jnp.int32), pltpu.VMEM((picks, toks), F32),
            pltpu.VMEM((toks, width), BF16),
            pltpu.VMEM((split, LANES), F32), pltpu.VMEM((split, LANES), F32),
            pltpu.VMEM((n * jc, LANES), F32),
            pltpu.VMEM((2, m, jc, LANES), BF16), pltpu.VMEM((n, jc, LANES), BF16),
            pltpu.VMEM((n, jc, LANES), BF16), pltpu.VMEM((n, jc, LANES), BF16),
            pltpu.VMEM((2 * low, width), BF16),
            pltpu.VMEM((total_rows, LANES), F32), pltpu.VMEM((others, total_rows, LANES), F32),
            pltpu.VMEM((padded, 2 * fs + LANES), F32), pltpu.VMEM((others, padded, 2 * fs + LANES), F32),
            pltpu.VMEM((m * cap, width), F32), pltpu.VMEM((padded, width), F32),
            dma((4,)), dma((6 * pieces,)),
            dma((2, m)), dma((n,)), dma((n,)), dma((n,)),
            dma((others * chunks * 3,)), dma((others * chunks * 3,)),
            dma((others * 3,)), dma((others * 3,)), dma((others,)), dma((others,)), dma((2,)), dma((2,)),
        ] + exchanged,
        compiler_params=pltpu.CompilerParams(
            collective_id=0, has_side_effects=True, vmem_limit_bytes=60 * 1024 * 1024
        ),
    )(tokens, norm_gain.reshape(1, width), routes.T, route_weights.T, eg, eu, ed, sg, su, sd)


def solution(mesh):
    placed = (
        P("ep", "tp"),
        P("tp"),
        P("ep", None),
        P("ep", None),
        P("ep", "tp", None),
        P("ep", "tp", None),
        P("ep", None, "tp"),
        P("tp", None),
        P("tp", None),
        P(None, "tp"),
    )
    return jax.shard_map(
        local, mesh=mesh, in_specs=placed, out_specs=P("ep", "tp"), check_vma=False
    )
```

```python
import functools

import jax
import jax.numpy as jnp
from jax import lax
from jax.experimental import pallas as pl
from jax.experimental.pallas import tpu as pltpu
from jax.sharding import PartitionSpec as P

MESH = pl.DeviceIdType.MESH
F32 = jnp.float32
BF16 = jnp.bfloat16
LANES = 128
TN = (((0,), (0,)), ((), ()))


def silu_mul(g, u):
    return g / (1.0 + jnp.exp(-g)) * u


def kernel(
    n, tp, cap, chunks,
    x_hbm, gain_hbm, routes_hbm, rw_hbm,
    eg_hbm, eu_hbm, ed_hbm, sg_hbm, su_hbm, sd_hbm,
    out_ref,
    wgu, wd, vg, vu, vd,
    x_ref, gain_ref, routes_ref, rw_ref, xm_ref, meta, metam,
    packed, outbuf, arrive, retbuf, back,
    rows, hid, squares, sssend, ssrecv, shsend, shrecv, acc, shout,
    isem, wsem, dsend, drecv, rsend, rrecv, tsend, trecv, qsend, qrecv, hsend, hrecv, xsend, xrecv, asend, arecv,
    *exchanged,
):
    me = lax.axis_index("ep")
    my_tp = lax.axis_index("tp")
    m, quarter = n // 2, n // 4
    half, inner = me // m, lax.rem(me, m)
    mirror = lax.rem(me + m, n)
    spot = lax.rem(me, quarter)
    bit = lax.rem(me // quarter, 2)
    split_ff = tp == 2
    early = me // quarter == 1
    theirs = 1 - my_tp
    toks, width = x_ref.shape
    picks = routes_ref.shape[0]
    ff = wd.shape[0]
    fs = vg.shape[1]
    blocks = width // LANES
    jc = blocks * cap
    cols = ff // chunks
    mine, psend, precv = exchanged[0::3], exchanged[1::3], exchanged[2::3]

    def mate(i):
        return half * m + lax.rem(inner + i, m)

    def in_quarter(q):
        return [q * quarter + lax.rem(spot + i, quarter) for i in range(quarter)]

    near = [mate(i) for i in range(m)]
    groups = [near, in_quarter(2 * (1 - half)), in_quarter(2 * (1 - half) + 1)]

    barrier = pltpu.get_barrier_semaphore()
    pl.semaphore_signal(barrier, inc=1, device_id={"ep": mirror}, device_id_type=MESH)
    for i in range(1, m):
        pl.semaphore_signal(barrier, inc=1, device_id={"ep": mate(i)}, device_id_type=MESH)
    for i in range(1, tp):
        pl.semaphore_signal(barrier, inc=1, device_id={"tp": lax.rem(my_tp + i, tp)}, device_id_type=MESH)

    small = []
    for i, (src, dst) in enumerate(
        ((routes_hbm, routes_ref), (rw_hbm, rw_ref), (x_hbm, x_ref), (gain_hbm, gain_ref))
    ):
        c = pltpu.make_async_copy(src, dst, isem.at[i])
        c.start()
        small.append(c)
    for c in small:
        c.wait()
    loads = {}
    parts = [("sg", sg_hbm, vg), ("su", su_hbm, vu)]
    for c in range(chunks):
        which = (theirs, my_tp)[c] if split_ff else c
        taken = pl.ds(pl.multiple_of(which * cols, LANES), cols)
        parts.append((f"e{c}", eg_hbm.at[0, :, taken], wgu.at[which, :, 0:cols]))
        parts.append((f"e{c}", eu_hbm.at[0, :, taken], wgu.at[which, :, cols : 2 * cols]))
    parts += [("ed", ed_hbm.at[0], wd), ("sd", sd_hbm, vd)]
    for slot, (name, src, dst) in enumerate(parts):
        c = pltpu.make_async_copy(src, dst, wsem.at[slot])
        c.start()
        loads.setdefault(name, []).append(c)

    def loaded(*names):
        for name in names:
            for c in loads[name]:
                c.wait()

    def places(routes, base, number):
        expert = lax.broadcasted_iota(jnp.int32, (number, toks), 0) + base
        hits = [routes[k : k + 1, :] == expert for k in range(picks)]
        named = jnp.zeros((number, toks), F32)
        for hit in hits:
            named = named + jnp.where(hit, 1.0, 0.0)
        row_i = lax.broadcasted_iota(jnp.int32, (toks, toks), 0)
        col_i = lax.broadcasted_iota(jnp.int32, (toks, toks), 1)
        earlier = jnp.where(row_i < col_i, 1.0, 0.0).astype(BF16)
        before = jnp.dot(named.astype(BF16), earlier, preferred_element_type=F32)
        return hits, jnp.where(named > 0.5, before, -1.0)

    def by_slot(place, v):
        return jnp.concatenate([jnp.where(place == s, v, 0.0) for s in range(cap)], axis=0).astype(BF16)

    def pack(value, j, number):
        for s in range(cap):
            packed[pl.ds(j * cap + s, number, stride=jc), :] = value[s * number : (s + 1) * number, :]

    def unpack(j, number):
        return jnp.concatenate(
            [packed[pl.ds(j * cap + s, number, stride=jc), :] for s in range(cap)], axis=0
        )

    def select_rows(g, routes, x):
        select = by_slot(places(routes, half * m, m)[1], 1.0)
        for j in range(blocks):
            cut = slice(j * LANES, (j + 1) * LANES)
            pack(jnp.dot(select, x[:, cut], preferred_element_type=F32), j, m)
        for p in range(m):
            outbuf[g, p] = packed[pl.ds(p * jc, jc), :].astype(BF16)

    pending = []

    def to_tp(src, dst_of, send_of, recv_of):
        copies = []
        for i in range(1, tp):
            c = pltpu.make_async_remote_copy(
                src_ref=src, dst_ref=dst_of(i - 1), send_sem=send_of(i - 1), recv_sem=recv_of(i - 1),
                device_id={"tp": lax.rem(my_tp + i, tp)}, device_id_type=MESH,
            )
            c.start()
            copies.append(c)
        pending.extend(copies)
        return copies

    def to_mirror(src, dst, at):
        c = pltpu.make_async_remote_copy(
            src_ref=src, dst_ref=dst, send_sem=xsend.at[at], recv_sem=xrecv.at[at],
            device_id={"ep": mirror}, device_id_type=MESH,
        )
        c.start()
        pending.append(c)
        return c

    def token_copies(g, home):
        for i in range(1, m):
            to = lax.rem(inner + i, m)
            pltpu.make_async_remote_copy(
                src_ref=outbuf.at[g, to], dst_ref=arrive.at[home], send_sem=dsend.at[g],
                recv_sem=drecv.at[g * (1 + bit)], device_id={"ep": mate(i)}, device_id_type=MESH,
            ).start()
        arrive[home] = outbuf[g, inner]

    def many(ref, number, send, recv):
        part = ref.at[pl.ds(0, number)]
        return pltpu.make_async_remote_copy(
            src_ref=part, dst_ref=part, send_sem=send, recv_sem=recv,
            device_id={"ep": mirror}, device_id_type=MESH,
        )

    def wait_tokens(g):
        if g == 0:
            many(arrive, m - 1, dsend.at[0], drecv.at[0]).wait_recv()
            return

        @pl.when(bit == g - 1)
        def _():
            many(arrive, quarter - 1, dsend.at[0], drecv.at[g]).wait_recv()

        @pl.when(bit != g - 1)
        def _():
            many(arrive, quarter, dsend.at[0], drecv.at[g]).wait_recv()

    def send_back(g):
        for i, home in enumerate(groups[g]):
            if g or i:
                pltpu.make_async_remote_copy(
                    src_ref=retbuf.at[home], dst_ref=back.at[me], send_sem=rsend.at[g],
                    recv_sem=rrecv.at[1 + bit if g else 0], device_id={"ep": home}, device_id_type=MESH,
                ).start()

    def returned(g):
        return many(back, quarter if g else m - 1, rsend.at[g], rrecv.at[g])

    routes = routes_ref[...]
    meta[0:picks, 0:toks] = routes.astype(F32)
    x = x_ref[...]
    gain = gain_ref[...]
    select_rows(0, routes, x)
    pl.semaphore_wait(barrier, m + tp - 1)
    mcopy = to_mirror(meta, metam, 1)
    xcopy = to_mirror(x_ref, xm_ref, 0)
    token_copies(0, me)
    rw = rw_ref[...]
    scaled = 2.5 * rw / jnp.sum(rw, axis=0, keepdims=True)

    def combiner(base):
        hits, place = places(routes, base, m)
        weight = jnp.zeros((m, toks), F32)
        for k in range(picks):
            weight = weight + jnp.where(hits[k], scaled[k : k + 1, :], 0.0)
        w_hi = weight.astype(BF16).astype(F32)
        return by_slot(place, w_hi), by_slot(place, weight - w_hi)

    combiners = combiner(half * m), combiner((1 - half) * m)
    rows[...] = jnp.zeros(rows.shape, BF16)
    xf = x.astype(F32)
    xg = (xf * gain).astype(BF16)
    ss_own = jnp.sum(xf * xf, axis=1, keepdims=True)
    shsend[...] = jnp.zeros(shsend.shape, F32)
    shsend[0:toks, 2 * fs : 2 * fs + LANES] = jnp.broadcast_to(ss_own, (toks, LANES))
    for name, w, base in (("sg", vg, 0), ("su", vu, fs)):
        loaded(name)
        shsend[0:toks, base : base + fs] = jnp.dot(xg, w[...], preferred_element_type=F32)
    shared = to_tp(shsend, lambda i: shrecv.at[i], lambda i: hsend.at[i], lambda i: hrecv.at[i])
    mcopy.wait_recv()
    xcopy.wait_recv()
    select_rows(1, metam[0:picks, 0:toks].astype(jnp.int32), xm_ref[...])
    token_copies(1, mirror)

    def finish_shared(copies):
        loaded("sd")
        for c in copies:
            c.wait_recv()
        total = shsend[...]
        for i in range(tp - 1):
            total = total + shrecv[i]
        r_own = lax.rsqrt(total[:, 2 * fs : 2 * fs + 1] / (width * tp) + 1e-06)
        sh_hidden = silu_mul(total[:, 0:fs] * r_own, total[:, fs : 2 * fs] * r_own).astype(BF16)
        shout[...] = jnp.dot(sh_hidden, vd[...], preferred_element_type=F32)

    def first_half(g):
        number = len(groups[g])
        count = number * cap
        low = -(-count // 16) * 16
        wait_tokens(g)
        for i, home in enumerate(groups[g]):
            packed[pl.ds(i * jc, jc), :] = arrive[home].astype(F32)
        ss = jnp.zeros((count, LANES), F32)
        for j in range(blocks):
            cut = slice(j * LANES, (j + 1) * LANES)
            piece = unpack(j, number)
            ss = ss + piece * piece
            scaled_piece = piece * gain[:, cut]
            hi = scaled_piece.astype(BF16)
            rows[0:count, cut] = hi
            rows[low : low + count, cut] = (scaled_piece - hi.astype(F32)).astype(BF16)
        squares[0:count, :] = jnp.broadcast_to(jnp.sum(ss, axis=1, keepdims=True), (count, LANES))
        sssend[g] = squares[...].T[0:8, :]
        all_copies = [to_tp(
            sssend.at[g], lambda i: ssrecv.at[i, g],
            lambda i: qsend.at[i * len(groups) + g], lambda i: qrecv.at[i * len(groups) + g],
        )]
        taken_rows = rows[0 : 2 * low, :]
        for c in range(chunks):
            loaded_once(c)
            own = split_ff and g == 0 and c > 0
            which = (theirs, my_tp)[c] if split_ff else c
            v = jnp.dot(taken_rows, wgu[which], preferred_element_type=F32)
            v = v[0:count] + v[low : low + count]
            mine[g][c] = v
            if own:
                continue
            psend[g][c] = v.astype(BF16)
            at_sem = lambda i: (i * len(groups) + g) * chunks + c
            all_copies.append(to_tp(
                psend[g].at[c], lambda i: precv[g].at[i, c],
                lambda i: tsend.at[at_sem(i)], lambda i: trecv.at[at_sem(i)],
            ))
        return all_copies

    def scale(g, copies):
        for c in copies:
            c.wait_recv()
        ss_all = sssend[g]
        for i in range(tp - 1):
            ss_all = ss_all + ssrecv[i, g]
        r_all = lax.rsqrt(ss_all / (width * tp) + 1e-06)
        return jnp.broadcast_to(r_all[0:1, :], squares.shape[::-1]).T[0 : len(groups[g]) * cap, 0:1]

    def activate(both, r):
        return silu_mul(both[:, 0:cols] * r, both[:, cols : 2 * cols] * r).astype(BF16)

    def deliver(g, value_of):
        number = len(groups[g])
        for j in range(blocks):
            pack(value_of(slice(j * LANES, (j + 1) * LANES)), j, number)
        for i, home in enumerate(groups[g]):
            retbuf[home] = packed[pl.ds(i * jc, jc), :].astype(BF16)
        send_back(g)
        if g == 0:
            back[me] = retbuf[me]

    def hidden_copy():
        return pltpu.make_async_remote_copy(
            src_ref=hid.at[my_tp], dst_ref=hid.at[my_tp], send_sem=asend.at[0], recv_sem=arecv.at[0],
            device_id={"tp": theirs}, device_id_type=MESH,
        )

    def hidden_half(all_copies):
        r = scale(0, all_copies[0])
        for c in all_copies[1]:
            c.wait_recv()
        hid[my_tp] = activate(mine[0][1] + precv[0][0, 0].astype(F32), r)
        hidden_copy().start()

    def out_half():
        hidden_copy().wait_recv()
        acc[0 : m * cap, :] = jnp.dot(hid[0], wd[0:cols, :], preferred_element_type=F32)
        part = jnp.dot(hid[1], wd[cols : 2 * cols, :], preferred_element_type=F32)
        deliver(0, lambda cut: acc[0 : m * cap, cut] + part[:, cut])

    def second_half(g, all_copies):
        count = len(groups[g]) * cap
        r = scale(g, all_copies[0])
        for c in range(chunks):
            for copy in all_copies[1 + c]:
                copy.wait_recv()
            which = (my_tp, theirs)[c] if split_ff else c
            both = mine[g][1 - c if split_ff else c]
            for i in range(tp - 1):
                both = both + precv[g][i, c].astype(F32)
            hidden = activate(both, r)
            part = jnp.dot(hidden, wd[pl.ds(pl.multiple_of(which * cols, LANES), cols), :], preferred_element_type=F32)
            if c == 0:
                acc[0:count, :] = part
            elif c < chunks - 1:
                acc[0:count, :] += part
            else:
                deliver(g, lambda cut: acc[0:count, cut] + part[:, cut])

    fetched = set()

    def loaded_once(c):
        if c not in fetched:
            fetched.add(c)
            loaded(f"e{c}")

    state0 = first_half(0)
    if split_ff:
        pl.when(early)(lambda: hidden_half(state0))
    state1 = first_half(1)
    state2 = first_half(2)
    loaded("ed")
    if split_ff:
        pl.when(jnp.logical_not(early))(lambda: hidden_half(state0))
        pl.when(early)(out_half)
    else:
        second_half(0, state0)
    second_half(1, state1)
    second_half(2, state2)
    if split_ff:
        pl.when(jnp.logical_not(early))(out_half)
    finish_shared(shared)

    def combined(base, pair):
        for p in range(m):
            packed[pl.ds(p * jc, jc), :] = back[base + p].astype(F32)
        for j in range(blocks):
            cut = slice(j * LANES, (j + 1) * LANES)
            piece = unpack(j, m).astype(BF16)
            routed = lax.dot_general(pair[0], piece, TN, preferred_element_type=F32)
            yield cut, routed + lax.dot_general(pair[1], piece, TN, preferred_element_type=F32)

    returned(0).wait_recv()
    for cut, routed in combined(half * m, combiners[0]):
        shout[0:toks, cut] += routed
    returned(1).wait_recv()
    returned(2).wait_recv()
    for cut, routed in combined((1 - half) * m, combiners[1]):
        out_ref[:, cut] = (shout[0:toks, cut] + routed).astype(BF16)
    for c in pending:
        c.wait_send()
    for g in range(2):
        many(arrive, m - 1, dsend.at[g], drecv.at[g]).wait_send()
    for g in range(len(groups)):
        returned(g).wait_send()
    if split_ff:
        hidden_copy().wait_send()


def local(tokens, norm_gain, routes, route_weights, eg, eu, ed, sg, su, sd):
    toks, width = tokens.shape
    picks = routes.shape[1]
    n, tp = lax.axis_size("ep"), lax.axis_size("tp")
    cap = max(2, toks * picks // n + 1)
    ff, fs = eg.shape[2], sg.shape[1]
    chunks = 2
    m, quarter = n // 2, n // 4
    jc = width // LANES * cap
    low = -(-m * cap // 16) * 16
    padded = -(-toks // 16) * 16
    cols = ff // chunks
    others = max(1, tp - 1)
    split = -(-picks // 8) * 8
    sizes = (m, quarter, quarter)
    slots = -(-m * cap // LANES) * LANES
    exchanged = []
    for s in sizes:
        exchanged += [
            pltpu.VMEM((chunks, s * cap, 2 * cols), F32),
            pltpu.VMEM((chunks, s * cap, 2 * cols), BF16),
            pltpu.VMEM((others, chunks, s * cap, 2 * cols), BF16),
        ]
    hbm = pl.BlockSpec(memory_space=pl.ANY)
    dma = pltpu.SemaphoreType.DMA
    return pl.pallas_call(
        functools.partial(kernel, n, tp, cap, chunks),
        out_shape=pltpu.VMEM((toks, width), BF16),
        in_specs=[hbm] * 10,
        out_specs=pl.BlockSpec(memory_space=pltpu.VMEM),
        scratch_shapes=[
            pltpu.VMEM((chunks, width, 2 * cols), BF16), pltpu.VMEM((ff, width), BF16),
            pltpu.VMEM((width, fs), BF16), pltpu.VMEM((width, fs), BF16), pltpu.VMEM((fs, width), BF16),
            pltpu.VMEM((toks, width), BF16), pltpu.VMEM((1, width), F32),
            pltpu.VMEM((picks, toks), jnp.int32), pltpu.VMEM((picks, toks), F32),
            pltpu.VMEM((toks, width), BF16),
            pltpu.VMEM((split, LANES), F32), pltpu.VMEM((split, LANES), F32),
            pltpu.VMEM((n * jc, LANES), F32),
            pltpu.VMEM((2, m, jc, LANES), BF16), pltpu.VMEM((n, jc, LANES), BF16),
            pltpu.VMEM((n, jc, LANES), BF16), pltpu.VMEM((n, jc, LANES), BF16),
            pltpu.VMEM((2 * low, width), BF16), pltpu.VMEM((chunks, m * cap, cols), BF16),
            pltpu.VMEM((slots, LANES), F32),
            pltpu.VMEM((3, 8, slots), F32), pltpu.VMEM((others, 3, 8, slots), F32),
            pltpu.VMEM((padded, 2 * fs + LANES), F32), pltpu.VMEM((others, padded, 2 * fs + LANES), F32),
            pltpu.VMEM((m * cap, width), F32), pltpu.VMEM((padded, width), F32),
            dma((4,)), dma((4 + 2 * chunks,)),
            dma((2,)), dma((3,)), dma((3,)), dma((3,)),
            dma((others * chunks * 3,)), dma((others * chunks * 3,)),
            dma((others * 3,)), dma((others * 3,)), dma((others,)), dma((others,)), dma((2,)), dma((2,)),
            dma((1,)), dma((1,)),
        ] + exchanged,
        compiler_params=pltpu.CompilerParams(
            collective_id=0, has_side_effects=True, vmem_limit_bytes=60 * 1024 * 1024
        ),
    )(tokens, norm_gain.reshape(1, width), routes.T, route_weights.T, eg, eu, ed, sg, su, sd)


def solution(mesh):
    placed = (
        P("ep", "tp"),
        P("tp"),
        P("ep", None),
        P("ep", None),
        P("ep", "tp", None),
        P("ep", "tp", None),
        P("ep", None, "tp"),
        P("tp", None),
        P("tp", None),
        P(None, "tp"),
    )
    return jax.shard_map(
        local, mesh=mesh, in_specs=placed, out_specs=P("ep", "tp"), check_vma=False
    )
```

```python
import functools

import jax
import jax.numpy as jnp
from jax import lax
from jax.experimental import pallas as pl
from jax.experimental.pallas import tpu as pltpu
from jax.sharding import PartitionSpec as P

MESH = pl.DeviceIdType.MESH
F32 = jnp.float32
BF16 = jnp.bfloat16
LANES = 128
TN = (((0,), (0,)), ((), ()))


def silu_mul(g, u):
    return g / (1.0 + jnp.exp(-g)) * u


def kernel(
    n, tp, cap, chunks,
    x_hbm, gain_hbm, routes_hbm, rw_hbm,
    eg_hbm, eu_hbm, ed_hbm, sg_hbm, su_hbm, sd_hbm,
    out_ref,
    wgu, wd, vg, vu, vd,
    x_ref, gain_ref, routes_ref, rw_ref, xm_ref, meta, metam,
    packed, outbuf, arrive, retbuf, back,
    rows, hid, squares, sssend, ssrecv, shsend, shrecv, acc, shout,
    isem, wsem, dsend, drecv, rsend, rrecv, tsend, trecv, qsend, qrecv, hsend, hrecv, xsend, xrecv, asend, arecv,
    *exchanged,
):
    me = lax.axis_index("ep")
    my_tp = lax.axis_index("tp")
    m, quarter = n // 2, n // 4
    half, inner = me // m, lax.rem(me, m)
    mirror = lax.rem(me + m, n)
    spot = lax.rem(me, quarter)
    bit = lax.rem(me // quarter, 2)
    split_ff = tp == 2
    theirs = 1 - my_tp
    toks, width = x_ref.shape
    picks = routes_ref.shape[0]
    ff = wd.shape[0]
    fs = vg.shape[1]
    blocks = width // LANES
    jc = blocks * cap
    cols = ff // chunks
    mine, psend, precv = exchanged[0::3], exchanged[1::3], exchanged[2::3]

    def mate(i):
        return half * m + lax.rem(inner + i, m)

    def in_quarter(q):
        return [q * quarter + lax.rem(spot + i, quarter) for i in range(quarter)]

    near = [mate(i) for i in range(m)]
    groups = [near, in_quarter(3 * (1 - half)), in_quarter(2 - half)]
    mirror_group = 1 + lax.rem(bit + 1 - half, 2)
    group_there = 1 + lax.rem(bit + half, 2)

    barrier = pltpu.get_barrier_semaphore()
    pl.semaphore_signal(barrier, inc=1, device_id={"ep": mirror}, device_id_type=MESH)
    for i in range(1, m):
        pl.semaphore_signal(barrier, inc=1, device_id={"ep": mate(i)}, device_id_type=MESH)
    for i in range(1, tp):
        pl.semaphore_signal(barrier, inc=1, device_id={"tp": lax.rem(my_tp + i, tp)}, device_id_type=MESH)

    small = []
    for i, (src, dst) in enumerate(
        ((routes_hbm, routes_ref), (rw_hbm, rw_ref), (x_hbm, x_ref), (gain_hbm, gain_ref))
    ):
        c = pltpu.make_async_copy(src, dst, isem.at[i])
        c.start()
        small.append(c)
    for c in small:
        c.wait()
    loads = {}
    parts = [("sg", sg_hbm, vg), ("su", su_hbm, vu)]
    for c in range(chunks):
        which = (theirs, my_tp)[c] if split_ff else c
        taken = pl.ds(pl.multiple_of(which * cols, LANES), cols)
        parts.append((f"e{c}", eg_hbm.at[0, :, taken], wgu.at[which, :, 0:cols]))
        parts.append((f"e{c}", eu_hbm.at[0, :, taken], wgu.at[which, :, cols : 2 * cols]))
    parts += [("ed", ed_hbm.at[0], wd), ("sd", sd_hbm, vd)]
    for slot, (name, src, dst) in enumerate(parts):
        c = pltpu.make_async_copy(src, dst, wsem.at[slot])
        c.start()
        loads.setdefault(name, []).append(c)

    def loaded(*names):
        for name in names:
            for c in loads[name]:
                c.wait()

    def places(routes, base, number):
        expert = lax.broadcasted_iota(jnp.int32, (number, toks), 0) + base
        hits = [routes[k : k + 1, :] == expert for k in range(picks)]
        named = jnp.zeros((number, toks), F32)
        for hit in hits:
            named = named + jnp.where(hit, 1.0, 0.0)
        row_i = lax.broadcasted_iota(jnp.int32, (toks, toks), 0)
        col_i = lax.broadcasted_iota(jnp.int32, (toks, toks), 1)
        earlier = jnp.where(row_i < col_i, 1.0, 0.0).astype(BF16)
        before = jnp.dot(named.astype(BF16), earlier, preferred_element_type=F32)
        return hits, jnp.where(named > 0.5, before, -1.0)

    def by_slot(place, v):
        return jnp.concatenate([jnp.where(place == s, v, 0.0) for s in range(cap)], axis=0).astype(BF16)

    def pack(value, j, number):
        for s in range(cap):
            packed[pl.ds(j * cap + s, number, stride=jc), :] = value[s * number : (s + 1) * number, :]

    def unpack(j, number):
        return jnp.concatenate(
            [packed[pl.ds(j * cap + s, number, stride=jc), :] for s in range(cap)], axis=0
        )

    def select_rows(g, routes, x):
        select = by_slot(places(routes, half * m, m)[1], 1.0)
        for j in range(blocks):
            cut = slice(j * LANES, (j + 1) * LANES)
            pack(jnp.dot(select, x[:, cut], preferred_element_type=F32), j, m)
        for p in range(m):
            outbuf[g, p] = packed[pl.ds(p * jc, jc), :].astype(BF16)

    pending = []

    def to_tp(src, dst_of, send_of, recv_of):
        copies = []
        for i in range(1, tp):
            c = pltpu.make_async_remote_copy(
                src_ref=src, dst_ref=dst_of(i - 1), send_sem=send_of(i - 1), recv_sem=recv_of(i - 1),
                device_id={"tp": lax.rem(my_tp + i, tp)}, device_id_type=MESH,
            )
            c.start()
            copies.append(c)
        pending.extend(copies)
        return copies

    def to_mirror(src, dst, at):
        c = pltpu.make_async_remote_copy(
            src_ref=src, dst_ref=dst, send_sem=xsend.at[at], recv_sem=xrecv.at[at],
            device_id={"ep": mirror}, device_id_type=MESH,
        )
        c.start()
        pending.append(c)
        return c

    def token_copies(g, home):
        for i in range(1, m):
            to = lax.rem(inner + i, m)
            pltpu.make_async_remote_copy(
                src_ref=outbuf.at[g, to], dst_ref=arrive.at[home], send_sem=dsend.at[g],
                recv_sem=drecv.at[g * mirror_group], device_id={"ep": mate(i)}, device_id_type=MESH,
            ).start()
        arrive[home] = outbuf[g, inner]

    def many(ref, number, send, recv):
        part = ref.at[pl.ds(0, number)]
        return pltpu.make_async_remote_copy(
            src_ref=part, dst_ref=part, send_sem=send, recv_sem=recv,
            device_id={"ep": mirror}, device_id_type=MESH,
        )

    def wait_tokens(g):
        if g == 0:
            many(arrive, m - 1, dsend.at[0], drecv.at[0]).wait_recv()
            return

        @pl.when(mirror_group == g)
        def _():
            many(arrive, quarter - 1, dsend.at[0], drecv.at[g]).wait_recv()

        @pl.when(mirror_group != g)
        def _():
            many(arrive, quarter, dsend.at[0], drecv.at[g]).wait_recv()

    def send_back(g):
        for i, home in enumerate(groups[g]):
            if g or i:
                pltpu.make_async_remote_copy(
                    src_ref=retbuf.at[home], dst_ref=back.at[me], send_sem=rsend.at[g],
                    recv_sem=rrecv.at[group_there if g else 0], device_id={"ep": home}, device_id_type=MESH,
                ).start()

    def returned(g):
        return many(back, quarter if g else m - 1, rsend.at[g], rrecv.at[g])

    routes = routes_ref[...]
    meta[0:picks, 0:toks] = routes.astype(F32)
    x = x_ref[...]
    gain = gain_ref[...]
    select_rows(0, routes, x)
    pl.semaphore_wait(barrier, m + tp - 1)
    mcopy = to_mirror(meta, metam, 1)
    xcopy = to_mirror(x_ref, xm_ref, 0)
    token_copies(0, me)
    rw = rw_ref[...]
    scaled = 2.5 * rw / jnp.sum(rw, axis=0, keepdims=True)

    def combiner(base):
        hits, place = places(routes, base, m)
        weight = jnp.zeros((m, toks), F32)
        for k in range(picks):
            weight = weight + jnp.where(hits[k], scaled[k : k + 1, :], 0.0)
        w_hi = weight.astype(BF16).astype(F32)
        return by_slot(place, w_hi), by_slot(place, weight - w_hi)

    combiners = combiner(half * m), combiner((1 - half) * m)
    rows[...] = jnp.zeros(rows.shape, BF16)
    xf = x.astype(F32)
    xg = (xf * gain).astype(BF16)
    ss_own = jnp.sum(xf * xf, axis=1, keepdims=True)
    shsend[...] = jnp.zeros(shsend.shape, F32)
    shsend[0:toks, 2 * fs : 2 * fs + LANES] = jnp.broadcast_to(ss_own, (toks, LANES))
    for name, w, base in (("sg", vg, 0), ("su", vu, fs)):
        loaded(name)
        shsend[0:toks, base : base + fs] = jnp.dot(xg, w[...], preferred_element_type=F32)
    shared = to_tp(shsend, lambda i: shrecv.at[i], lambda i: hsend.at[i], lambda i: hrecv.at[i])
    mcopy.wait_recv()
    xcopy.wait_recv()
    select_rows(1, metam[0:picks, 0:toks].astype(jnp.int32), xm_ref[...])
    token_copies(1, mirror)

    def finish_shared(copies):
        loaded("sd")
        for c in copies:
            c.wait_recv()
        total = shsend[...]
        for i in range(tp - 1):
            total = total + shrecv[i]
        r_own = lax.rsqrt(total[:, 2 * fs : 2 * fs + 1] / (width * tp) + 1e-06)
        sh_hidden = silu_mul(total[:, 0:fs] * r_own, total[:, fs : 2 * fs] * r_own).astype(BF16)
        shout[...] = jnp.dot(sh_hidden, vd[...], preferred_element_type=F32)

    def first_half(g):
        number = len(groups[g])
        count = number * cap
        low = -(-count // 16) * 16
        wait_tokens(g)
        for i, home in enumerate(groups[g]):
            packed[pl.ds(i * jc, jc), :] = arrive[home].astype(F32)
        ss = jnp.zeros((count, LANES), F32)
        for j in range(blocks):
            cut = slice(j * LANES, (j + 1) * LANES)
            piece = unpack(j, number)
            ss = ss + piece * piece
            scaled_piece = piece * gain[:, cut]
            hi = scaled_piece.astype(BF16)
            rows[0:count, cut] = hi
            rows[low : low + count, cut] = (scaled_piece - hi.astype(F32)).astype(BF16)
        squares[0:count, :] = jnp.broadcast_to(jnp.sum(ss, axis=1, keepdims=True), (count, LANES))
        sssend[g] = squares[...].T[0:8, :]
        all_copies = [to_tp(
            sssend.at[g], lambda i: ssrecv.at[i, g],
            lambda i: qsend.at[i * len(groups) + g], lambda i: qrecv.at[i * len(groups) + g],
        )]
        taken_rows = rows[0 : 2 * low, :]
        for c in range(chunks):
            loaded_once(c)
            own = split_ff and g == 0 and c > 0
            which = (theirs, my_tp)[c] if split_ff else c
            v = jnp.dot(taken_rows, wgu[which], preferred_element_type=F32)
            v = v[0:count] + v[low : low + count]
            mine[g][c] = v
            if own:
                continue
            psend[g][c] = v.astype(BF16)
            at_sem = lambda i: (i * len(groups) + g) * chunks + c
            all_copies.append(to_tp(
                psend[g].at[c], lambda i: precv[g].at[i, c],
                lambda i: tsend.at[at_sem(i)], lambda i: trecv.at[at_sem(i)],
            ))
        return all_copies

    def scale(g, copies):
        for c in copies:
            c.wait_recv()
        ss_all = sssend[g]
        for i in range(tp - 1):
            ss_all = ss_all + ssrecv[i, g]
        r_all = lax.rsqrt(ss_all / (width * tp) + 1e-06)
        return jnp.broadcast_to(r_all[0:1, :], squares.shape[::-1]).T[0 : len(groups[g]) * cap, 0:1]

    def activate(both, r):
        return silu_mul(both[:, 0:cols] * r, both[:, cols : 2 * cols] * r).astype(BF16)

    def deliver(g, value_of):
        number = len(groups[g])
        for j in range(blocks):
            pack(value_of(slice(j * LANES, (j + 1) * LANES)), j, number)
        for i, home in enumerate(groups[g]):
            retbuf[home] = packed[pl.ds(i * jc, jc), :].astype(BF16)
        send_back(g)
        if g == 0:
            back[me] = retbuf[me]

    def hidden_copy():
        return pltpu.make_async_remote_copy(
            src_ref=hid.at[my_tp], dst_ref=hid.at[my_tp], send_sem=asend.at[0], recv_sem=arecv.at[0],
            device_id={"tp": theirs}, device_id_type=MESH,
        )

    def hidden_half(all_copies):
        r = scale(0, all_copies[0])
        for c in all_copies[1]:
            c.wait_recv()
        hid[my_tp] = activate(mine[0][1] + precv[0][0, 0].astype(F32), r)
        hidden_copy().start()

    def out_half():
        hidden_copy().wait_recv()
        acc[0 : m * cap, :] = jnp.dot(hid[0], wd[0:cols, :], preferred_element_type=F32)
        part = jnp.dot(hid[1], wd[cols : 2 * cols, :], preferred_element_type=F32)
        deliver(0, lambda cut: acc[0 : m * cap, cut] + part[:, cut])

    def second_half(g, all_copies):
        count = len(groups[g]) * cap
        r = scale(g, all_copies[0])
        for c in range(chunks):
            for copy in all_copies[1 + c]:
                copy.wait_recv()
            which = (my_tp, theirs)[c] if split_ff else c
            both = mine[g][1 - c if split_ff else c]
            for i in range(tp - 1):
                both = both + precv[g][i, c].astype(F32)
            hidden = activate(both, r)
            part = jnp.dot(hidden, wd[pl.ds(pl.multiple_of(which * cols, LANES), cols), :], preferred_element_type=F32)
            if c == 0:
                acc[0:count, :] = part
            elif c < chunks - 1:
                acc[0:count, :] += part
            else:
                deliver(g, lambda cut: acc[0:count, cut] + part[:, cut])

    fetched = set()

    def loaded_once(c):
        if c not in fetched:
            fetched.add(c)
            loaded(f"e{c}")

    def only(where, step):
        if split_ff:
            pl.when(where)(step)

    lower, upper = half == 0, half == 1
    state0 = first_half(0)
    state1 = first_half(1)
    only(lower, lambda: hidden_half(state0))
    state2 = first_half(2)
    only(upper, lambda: hidden_half(state0))
    loaded("ed")
    if not split_ff:
        second_half(0, state0)
    second_half(1, state1)
    only(lower, out_half)
    second_half(2, state2)
    only(upper, out_half)
    finish_shared(shared)

    def combined(base, pair):
        for p in range(m):
            packed[pl.ds(p * jc, jc), :] = back[base + p].astype(F32)
        for j in range(blocks):
            cut = slice(j * LANES, (j + 1) * LANES)
            piece = unpack(j, m).astype(BF16)
            routed = lax.dot_general(pair[0], piece, TN, preferred_element_type=F32)
            yield cut, routed + lax.dot_general(pair[1], piece, TN, preferred_element_type=F32)

    returned(0).wait_recv()
    for cut, routed in combined(half * m, combiners[0]):
        shout[0:toks, cut] += routed
    returned(1).wait_recv()
    returned(2).wait_recv()
    for cut, routed in combined((1 - half) * m, combiners[1]):
        out_ref[:, cut] = (shout[0:toks, cut] + routed).astype(BF16)
    for c in pending:
        c.wait_send()
    for g in range(2):
        many(arrive, m - 1, dsend.at[g], drecv.at[g]).wait_send()
    for g in range(len(groups)):
        returned(g).wait_send()
    if split_ff:
        hidden_copy().wait_send()


def local(tokens, norm_gain, routes, route_weights, eg, eu, ed, sg, su, sd):
    toks, width = tokens.shape
    picks = routes.shape[1]
    n, tp = lax.axis_size("ep"), lax.axis_size("tp")
    cap = max(2, toks * picks // n + 1)
    ff, fs = eg.shape[2], sg.shape[1]
    chunks = 2
    m, quarter = n // 2, n // 4
    jc = width // LANES * cap
    low = -(-m * cap // 16) * 16
    padded = -(-toks // 16) * 16
    cols = ff // chunks
    others = max(1, tp - 1)
    split = -(-picks // 8) * 8
    sizes = (m, quarter, quarter)
    slots = -(-m * cap // LANES) * LANES
    exchanged = []
    for s in sizes:
        exchanged += [
            pltpu.VMEM((chunks, s * cap, 2 * cols), F32),
            pltpu.VMEM((chunks, s * cap, 2 * cols), BF16),
            pltpu.VMEM((others, chunks, s * cap, 2 * cols), BF16),
        ]
    hbm = pl.BlockSpec(memory_space=pl.ANY)
    dma = pltpu.SemaphoreType.DMA
    return pl.pallas_call(
        functools.partial(kernel, n, tp, cap, chunks),
        out_shape=pltpu.VMEM((toks, width), BF16),
        in_specs=[hbm] * 10,
        out_specs=pl.BlockSpec(memory_space=pltpu.VMEM),
        scratch_shapes=[
            pltpu.VMEM((chunks, width, 2 * cols), BF16), pltpu.VMEM((ff, width), BF16),
            pltpu.VMEM((width, fs), BF16), pltpu.VMEM((width, fs), BF16), pltpu.VMEM((fs, width), BF16),
            pltpu.VMEM((toks, width), BF16), pltpu.VMEM((1, width), F32),
            pltpu.VMEM((picks, toks), jnp.int32), pltpu.VMEM((picks, toks), F32),
            pltpu.VMEM((toks, width), BF16),
            pltpu.VMEM((split, LANES), F32), pltpu.VMEM((split, LANES), F32),
            pltpu.VMEM((n * jc, LANES), F32),
            pltpu.VMEM((2, m, jc, LANES), BF16), pltpu.VMEM((n, jc, LANES), BF16),
            pltpu.VMEM((n, jc, LANES), BF16), pltpu.VMEM((n, jc, LANES), BF16),
            pltpu.VMEM((2 * low, width), BF16), pltpu.VMEM((chunks, m * cap, cols), BF16),
            pltpu.VMEM((slots, LANES), F32),
            pltpu.VMEM((3, 8, slots), F32), pltpu.VMEM((others, 3, 8, slots), F32),
            pltpu.VMEM((padded, 2 * fs + LANES), F32), pltpu.VMEM((others, padded, 2 * fs + LANES), F32),
            pltpu.VMEM((m * cap, width), F32), pltpu.VMEM((padded, width), F32),
            dma((4,)), dma((4 + 2 * chunks,)),
            dma((2,)), dma((3,)), dma((3,)), dma((3,)),
            dma((others * chunks * 3,)), dma((others * chunks * 3,)),
            dma((others * 3,)), dma((others * 3,)), dma((others,)), dma((others,)), dma((2,)), dma((2,)),
            dma((1,)), dma((1,)),
        ] + exchanged,
        compiler_params=pltpu.CompilerParams(
            collective_id=0, has_side_effects=True, vmem_limit_bytes=60 * 1024 * 1024
        ),
    )(tokens, norm_gain.reshape(1, width), routes.T, route_weights.T, eg, eu, ed, sg, su, sd)


def solution(mesh):
    placed = (
        P("ep", "tp"),
        P("tp"),
        P("ep", None),
        P("ep", None),
        P("ep", "tp", None),
        P("ep", "tp", None),
        P("ep", None, "tp"),
        P("tp", None),
        P("tp", None),
        P(None, "tp"),
    )
    return jax.shard_map(
        local, mesh=mesh, in_specs=placed, out_specs=P("ep", "tp"), check_vma=False
    )
```

```python
import functools

import jax
import jax.numpy as jnp
from jax import lax
from jax.experimental import pallas as pl
from jax.experimental.pallas import tpu as pltpu
from jax.sharding import PartitionSpec as P

MESH = pl.DeviceIdType.MESH
F32 = jnp.float32
BF16 = jnp.bfloat16
LANES = 128
TN = (((0,), (0,)), ((), ()))


def silu_mul(g, u):
    return g / (1.0 + jnp.exp(-g)) * u


def kernel(
    n, tp, cap, chunks,
    x_hbm, gain_hbm, routes_hbm, rw_hbm,
    eg_hbm, eu_hbm, ed_hbm, sg_hbm, su_hbm, sd_hbm,
    out_ref,
    wgu, wd, vg, vu, vd,
    x_ref, gain_ref, routes_ref, rw_ref, xm_ref, meta, metam,
    packed, outbuf, arrive, retbuf, back,
    rows, hid, squares, sssend, ssrecv, shsend, shrecv, acc, shout,
    isem, wsem, dsend, drecv, rsend, rrecv, tsend, trecv, qsend, qrecv, hsend, hrecv, xsend, xrecv, asend, arecv,
    *exchanged,
):
    me = lax.axis_index("ep")
    my_tp = lax.axis_index("tp")
    m, quarter = n // 2, n // 4
    half, inner = me // m, lax.rem(me, m)
    mirror = lax.rem(me + m, n)
    spot = lax.rem(me, quarter)
    bit = lax.rem(me // quarter, 2)
    split_ff = tp == 2
    theirs = 1 - my_tp
    toks, width = x_ref.shape
    picks = routes_ref.shape[0]
    ff = wd.shape[0]
    fs = vg.shape[1]
    blocks = width // LANES
    jc = blocks * cap
    cols = ff // chunks
    mine, psend, precv = exchanged[0::3], exchanged[1::3], exchanged[2::3]

    def mate(i):
        return half * m + lax.rem(inner + i, m)

    def in_quarter(q):
        return [q * quarter + i for i in range(quarter)]

    near = [mate(i) for i in range(m)]
    groups = [near, in_quarter(3 * (1 - half)), in_quarter(2 - half)]
    mirror_group = 1 + lax.rem(bit + 1 - half, 2)
    group_there = 1 + lax.rem(bit + half, 2)

    barrier = pltpu.get_barrier_semaphore()
    pl.semaphore_signal(barrier, inc=1, device_id={"ep": mirror}, device_id_type=MESH)
    for i in range(1, m):
        pl.semaphore_signal(barrier, inc=1, device_id={"ep": mate(i)}, device_id_type=MESH)
    for i in range(1, tp):
        pl.semaphore_signal(barrier, inc=1, device_id={"tp": lax.rem(my_tp + i, tp)}, device_id_type=MESH)

    small = []
    for i, (src, dst) in enumerate(
        ((routes_hbm, routes_ref), (rw_hbm, rw_ref), (x_hbm, x_ref), (gain_hbm, gain_ref))
    ):
        c = pltpu.make_async_copy(src, dst, isem.at[i])
        c.start()
        small.append(c)
    for c in small:
        c.wait()
    loads = {}
    parts = [("sg", sg_hbm, vg), ("su", su_hbm, vu)]
    for c in range(chunks):
        which = (theirs, my_tp)[c] if split_ff else c
        taken = pl.ds(pl.multiple_of(which * cols, LANES), cols)
        parts.append((f"e{c}", eg_hbm.at[0, :, taken], wgu.at[which, :, 0:cols]))
        parts.append((f"e{c}", eu_hbm.at[0, :, taken], wgu.at[which, :, cols : 2 * cols]))
    parts += [("ed", ed_hbm.at[0], wd), ("sd", sd_hbm, vd)]
    for slot, (name, src, dst) in enumerate(parts):
        c = pltpu.make_async_copy(src, dst, wsem.at[slot])
        c.start()
        loads.setdefault(name, []).append(c)

    def loaded(*names):
        for name in names:
            for c in loads[name]:
                c.wait()

    def places(routes, base, number):
        expert = lax.broadcasted_iota(jnp.int32, (number, toks), 0) + base
        hits = [routes[k : k + 1, :] == expert for k in range(picks)]
        named = jnp.zeros((number, toks), F32)
        for hit in hits:
            named = named + jnp.where(hit, 1.0, 0.0)
        row_i = lax.broadcasted_iota(jnp.int32, (toks, toks), 0)
        col_i = lax.broadcasted_iota(jnp.int32, (toks, toks), 1)
        earlier = jnp.where(row_i < col_i, 1.0, 0.0).astype(BF16)
        before = jnp.dot(named.astype(BF16), earlier, preferred_element_type=F32)
        return hits, jnp.where(named > 0.5, before, -1.0)

    def by_slot(place, v):
        return jnp.concatenate([jnp.where(place == s, v, 0.0) for s in range(cap)], axis=0).astype(BF16)

    def pack(value, j, number):
        for s in range(cap):
            packed[pl.ds(j * cap + s, number, stride=jc), :] = value[s * number : (s + 1) * number, :]

    def unpack(j, number):
        return jnp.concatenate(
            [packed[pl.ds(j * cap + s, number, stride=jc), :] for s in range(cap)], axis=0
        )

    def select_rows(g, routes, x):
        select = by_slot(places(routes, half * m, m)[1], 1.0)
        for j in range(blocks):
            cut = slice(j * LANES, (j + 1) * LANES)
            pack(jnp.dot(select, x[:, cut], preferred_element_type=F32), j, m)
        for p in range(m):
            outbuf[g, p] = packed[pl.ds(p * jc, jc), :].astype(BF16)

    pending = []

    def to_tp(src, dst_of, send_of, recv_of):
        copies = []
        for i in range(1, tp):
            c = pltpu.make_async_remote_copy(
                src_ref=src, dst_ref=dst_of(i - 1), send_sem=send_of(i - 1), recv_sem=recv_of(i - 1),
                device_id={"tp": lax.rem(my_tp + i, tp)}, device_id_type=MESH,
            )
            c.start()
            copies.append(c)
        pending.extend(copies)
        return copies

    def to_mirror(src, dst, at):
        c = pltpu.make_async_remote_copy(
            src_ref=src, dst_ref=dst, send_sem=xsend.at[at], recv_sem=xrecv.at[at],
            device_id={"ep": mirror}, device_id_type=MESH,
        )
        c.start()
        pending.append(c)
        return c

    def token_copies(g, home):
        for i in range(1, m):
            to = lax.rem(inner + i, m)
            pltpu.make_async_remote_copy(
                src_ref=outbuf.at[g, to], dst_ref=arrive.at[home], send_sem=dsend.at[g],
                recv_sem=drecv.at[g * mirror_group], device_id={"ep": mate(i)}, device_id_type=MESH,
            ).start()
        arrive[home] = outbuf[g, inner]

    def many(ref, number, send, recv):
        part = ref.at[pl.ds(0, number)]
        return pltpu.make_async_remote_copy(
            src_ref=part, dst_ref=part, send_sem=send, recv_sem=recv,
            device_id={"ep": mirror}, device_id_type=MESH,
        )

    def wait_tokens(g):
        if g == 0:
            many(arrive, m - 1, dsend.at[0], drecv.at[0]).wait_recv()
            return

        @pl.when(mirror_group == g)
        def _():
            many(arrive, quarter - 1, dsend.at[0], drecv.at[g]).wait_recv()

        @pl.when(mirror_group != g)
        def _():
            many(arrive, quarter, dsend.at[0], drecv.at[g]).wait_recv()

    def send_back(g):
        for i, home in enumerate(groups[g]):
            if g or i:
                pltpu.make_async_remote_copy(
                    src_ref=retbuf.at[home], dst_ref=back.at[me], send_sem=rsend.at[g],
                    recv_sem=rrecv.at[group_there if g else 0], device_id={"ep": home}, device_id_type=MESH,
                ).start()

    def returned(g):
        return many(back, quarter if g else m - 1, rsend.at[g], rrecv.at[g])

    routes = routes_ref[...]
    meta[0:picks, 0:toks] = routes.astype(F32)
    x = x_ref[...]
    gain = gain_ref[...]
    select_rows(0, routes, x)
    pl.semaphore_wait(barrier, m + tp - 1)
    mcopy = to_mirror(meta, metam, 1)
    xcopy = to_mirror(x_ref, xm_ref, 0)
    token_copies(0, me)
    rw = rw_ref[...]
    scaled = 2.5 * rw / jnp.sum(rw, axis=0, keepdims=True)

    def combiner(base, number):
        hits, place = places(routes, base, number)
        weight = jnp.zeros((number, toks), F32)
        for k in range(picks):
            weight = weight + jnp.where(hits[k], scaled[k : k + 1, :], 0.0)
        w_hi = weight.astype(BF16).astype(F32)
        return by_slot(place, w_hi), by_slot(place, weight - w_hi)

    bases = half * m, 3 * (1 - half) * quarter, (2 - half) * quarter
    combiners = [combiner(base, len(group)) for base, group in zip(bases, groups)]
    rows[...] = jnp.zeros(rows.shape, BF16)
    xf = x.astype(F32)
    xg = (xf * gain).astype(BF16)
    ss_own = jnp.sum(xf * xf, axis=1, keepdims=True)
    shsend[...] = jnp.zeros(shsend.shape, F32)
    shsend[0:toks, 2 * fs : 2 * fs + LANES] = jnp.broadcast_to(ss_own, (toks, LANES))
    for name, w, base in (("sg", vg, 0), ("su", vu, fs)):
        loaded(name)
        shsend[0:toks, base : base + fs] = jnp.dot(xg, w[...], preferred_element_type=F32)
    shared = to_tp(shsend, lambda i: shrecv.at[i], lambda i: hsend.at[i], lambda i: hrecv.at[i])
    def serve_mirror():
        mcopy.wait_recv()
        xcopy.wait_recv()
        select_rows(1, metam[0:picks, 0:toks].astype(jnp.int32), xm_ref[...])
        token_copies(1, mirror)

    pl.when(me >= quarter)(serve_mirror)

    def finish_shared(copies):
        loaded("sd")
        for c in copies:
            c.wait_recv()
        total = shsend[...]
        for i in range(tp - 1):
            total = total + shrecv[i]
        r_own = lax.rsqrt(total[:, 2 * fs : 2 * fs + 1] / (width * tp) + 1e-06)
        sh_hidden = silu_mul(total[:, 0:fs] * r_own, total[:, fs : 2 * fs] * r_own).astype(BF16)
        shout[...] = jnp.dot(sh_hidden, vd[...], preferred_element_type=F32)

    def first_half(g):
        number = len(groups[g])
        count = number * cap
        low = -(-count // 16) * 16
        wait_tokens(g)
        for i, home in enumerate(groups[g]):
            packed[pl.ds(i * jc, jc), :] = arrive[home].astype(F32)
        ss = jnp.zeros((count, LANES), F32)
        for j in range(blocks):
            cut = slice(j * LANES, (j + 1) * LANES)
            piece = unpack(j, number)
            ss = ss + piece * piece
            scaled_piece = piece * gain[:, cut]
            hi = scaled_piece.astype(BF16)
            rows[0:count, cut] = hi
            rows[low : low + count, cut] = (scaled_piece - hi.astype(F32)).astype(BF16)
        squares[0:count, :] = jnp.broadcast_to(jnp.sum(ss, axis=1, keepdims=True), (count, LANES))
        sssend[g] = squares[...].T[0:8, :]
        all_copies = [to_tp(
            sssend.at[g], lambda i: ssrecv.at[i, g],
            lambda i: qsend.at[i * len(groups) + g], lambda i: qrecv.at[i * len(groups) + g],
        )]
        taken_rows = rows[0 : 2 * low, :]
        for c in range(chunks):
            loaded_once(c)
            own = split_ff and g == 0 and c > 0
            which = (theirs, my_tp)[c] if split_ff else c
            v = jnp.dot(taken_rows, wgu[which], preferred_element_type=F32)
            v = v[0:count] + v[low : low + count]
            mine[g][c] = v
            if own:
                continue
            psend[g][c] = v.astype(BF16)
            at_sem = lambda i: (i * len(groups) + g) * chunks + c
            all_copies.append(to_tp(
                psend[g].at[c], lambda i: precv[g].at[i, c],
                lambda i: tsend.at[at_sem(i)], lambda i: trecv.at[at_sem(i)],
            ))
        return all_copies

    def scale(g, copies):
        for c in copies:
            c.wait_recv()
        ss_all = sssend[g]
        for i in range(tp - 1):
            ss_all = ss_all + ssrecv[i, g]
        r_all = lax.rsqrt(ss_all / (width * tp) + 1e-06)
        return jnp.broadcast_to(r_all[0:1, :], squares.shape[::-1]).T[0 : len(groups[g]) * cap, 0:1]

    def activate(both, r):
        return silu_mul(both[:, 0:cols] * r, both[:, cols : 2 * cols] * r).astype(BF16)

    def deliver(g, value_of):
        number = len(groups[g])
        for j in range(blocks):
            pack(value_of(slice(j * LANES, (j + 1) * LANES)), j, number)
        for i, home in enumerate(groups[g]):
            retbuf[home] = packed[pl.ds(i * jc, jc), :].astype(BF16)
        send_back(g)
        if g == 0:
            back[me] = retbuf[me]

    def hidden_copy():
        return pltpu.make_async_remote_copy(
            src_ref=hid.at[my_tp], dst_ref=hid.at[my_tp], send_sem=asend.at[0], recv_sem=arecv.at[0],
            device_id={"tp": theirs}, device_id_type=MESH,
        )

    def hidden_half(all_copies):
        r = scale(0, all_copies[0])
        for c in all_copies[1]:
            c.wait_recv()
        hid[my_tp] = activate(mine[0][1] + precv[0][0, 0].astype(F32), r)
        hidden_copy().start()

    def out_half():
        hidden_copy().wait_recv()
        acc[0 : m * cap, :] = jnp.dot(hid[0], wd[0:cols, :], preferred_element_type=F32)
        part = jnp.dot(hid[1], wd[cols : 2 * cols, :], preferred_element_type=F32)
        deliver(0, lambda cut: acc[0 : m * cap, cut] + part[:, cut])

    def second_half(g, all_copies):
        count = len(groups[g]) * cap
        r = scale(g, all_copies[0])
        for c in range(chunks):
            for copy in all_copies[1 + c]:
                copy.wait_recv()
            which = (my_tp, theirs)[c] if split_ff else c
            both = mine[g][1 - c if split_ff else c]
            for i in range(tp - 1):
                both = both + precv[g][i, c].astype(F32)
            hidden = activate(both, r)
            part = jnp.dot(hidden, wd[pl.ds(pl.multiple_of(which * cols, LANES), cols), :], preferred_element_type=F32)
            if c == 0:
                acc[0:count, :] = part
            elif c < chunks - 1:
                acc[0:count, :] += part
            else:
                deliver(g, lambda cut: acc[0:count, cut] + part[:, cut])

    fetched = set()

    def loaded_once(c):
        if c not in fetched:
            fetched.add(c)
            loaded(f"e{c}")

    def only(where, step):
        if split_ff:
            pl.when(where)(step)

    lower, upper = half == 0, half == 1
    state0 = first_half(0)
    pl.when(me < quarter)(serve_mirror)
    state1 = first_half(1)
    only(lower, lambda: hidden_half(state0))
    state2 = first_half(2)
    only(upper, lambda: hidden_half(state0))
    loaded("ed")
    if not split_ff:
        second_half(0, state0)
    second_half(1, state1)
    only(lower, out_half)
    second_half(2, state2)
    only(upper, out_half)
    finish_shared(shared)

    def combined(g):
        number = len(groups[g])
        for p in range(number):
            packed[pl.ds(p * jc, jc), :] = back[bases[g] + p].astype(F32)
        for j in range(blocks):
            cut = slice(j * LANES, (j + 1) * LANES)
            piece = unpack(j, number).astype(BF16)
            routed = lax.dot_general(combiners[g][0], piece, TN, preferred_element_type=F32)
            routed = routed + lax.dot_general(combiners[g][1], piece, TN, preferred_element_type=F32)
            yield cut, shout[0:toks, cut] + routed

    for g in range(len(groups)):
        returned(g).wait_recv()
        for cut, value in combined(g):
            if g < len(groups) - 1:
                shout[0:toks, cut] = value
            else:
                out_ref[:, cut] = value.astype(BF16)
    for c in pending:
        c.wait_send()
    for g in range(2):
        many(arrive, m - 1, dsend.at[g], drecv.at[g]).wait_send()
    for g in range(len(groups)):
        returned(g).wait_send()
    if split_ff:
        hidden_copy().wait_send()


def local(tokens, norm_gain, routes, route_weights, eg, eu, ed, sg, su, sd):
    toks, width = tokens.shape
    picks = routes.shape[1]
    n, tp = lax.axis_size("ep"), lax.axis_size("tp")
    cap = max(2, toks * picks // n + 1)
    ff, fs = eg.shape[2], sg.shape[1]
    chunks = 2
    m, quarter = n // 2, n // 4
    jc = width // LANES * cap
    low = -(-m * cap // 16) * 16
    padded = -(-toks // 16) * 16
    cols = ff // chunks
    others = max(1, tp - 1)
    split = -(-picks // 8) * 8
    sizes = (m, quarter, quarter)
    slots = -(-m * cap // LANES) * LANES
    exchanged = []
    for s in sizes:
        exchanged += [
            pltpu.VMEM((chunks, s * cap, 2 * cols), F32),
            pltpu.VMEM((chunks, s * cap, 2 * cols), BF16),
            pltpu.VMEM((others, chunks, s * cap, 2 * cols), BF16),
        ]
    hbm = pl.BlockSpec(memory_space=pl.ANY)
    dma = pltpu.SemaphoreType.DMA
    return pl.pallas_call(
        functools.partial(kernel, n, tp, cap, chunks),
        out_shape=pltpu.VMEM((toks, width), BF16),
        in_specs=[hbm] * 10,
        out_specs=pl.BlockSpec(memory_space=pltpu.VMEM),
        scratch_shapes=[
            pltpu.VMEM((chunks, width, 2 * cols), BF16), pltpu.VMEM((ff, width), BF16),
            pltpu.VMEM((width, fs), BF16), pltpu.VMEM((width, fs), BF16), pltpu.VMEM((fs, width), BF16),
            pltpu.VMEM((toks, width), BF16), pltpu.VMEM((1, width), F32),
            pltpu.VMEM((picks, toks), jnp.int32), pltpu.VMEM((picks, toks), F32),
            pltpu.VMEM((toks, width), BF16),
            pltpu.VMEM((split, LANES), F32), pltpu.VMEM((split, LANES), F32),
            pltpu.VMEM((n * jc, LANES), F32),
            pltpu.VMEM((2, m, jc, LANES), BF16), pltpu.VMEM((n, jc, LANES), BF16),
            pltpu.VMEM((n, jc, LANES), BF16), pltpu.VMEM((n, jc, LANES), BF16),
            pltpu.VMEM((2 * low, width), BF16), pltpu.VMEM((chunks, m * cap, cols), BF16),
            pltpu.VMEM((slots, LANES), F32),
            pltpu.VMEM((3, 8, slots), F32), pltpu.VMEM((others, 3, 8, slots), F32),
            pltpu.VMEM((padded, 2 * fs + LANES), F32), pltpu.VMEM((others, padded, 2 * fs + LANES), F32),
            pltpu.VMEM((m * cap, width), F32), pltpu.VMEM((padded, width), F32),
            dma((4,)), dma((4 + 2 * chunks,)),
            dma((2,)), dma((3,)), dma((3,)), dma((3,)),
            dma((others * chunks * 3,)), dma((others * chunks * 3,)),
            dma((others * 3,)), dma((others * 3,)), dma((others,)), dma((others,)), dma((2,)), dma((2,)),
            dma((1,)), dma((1,)),
        ] + exchanged,
        compiler_params=pltpu.CompilerParams(
            collective_id=0, has_side_effects=True, vmem_limit_bytes=60 * 1024 * 1024
        ),
    )(tokens, norm_gain.reshape(1, width), routes.T, route_weights.T, eg, eu, ed, sg, su, sd)


def solution(mesh):
    placed = (
        P("ep", "tp"),
        P("tp"),
        P("ep", None),
        P("ep", None),
        P("ep", "tp", None),
        P("ep", "tp", None),
        P("ep", None, "tp"),
        P("tp", None),
        P("tp", None),
        P(None, "tp"),
    )
    return jax.shard_map(
        local, mesh=mesh, in_specs=placed, out_specs=P("ep", "tp"), check_vma=False
    )
```

```python
import functools

import jax
import jax.numpy as jnp
from jax import lax
from jax.experimental import pallas as pl
from jax.experimental.pallas import tpu as pltpu
from jax.sharding import PartitionSpec as P

MESH = pl.DeviceIdType.MESH
F32 = jnp.float32
BF16 = jnp.bfloat16
LANES = 128
TN = (((0,), (0,)), ((), ()))


def silu_mul(g, u):
    return g / (1.0 + jnp.exp(-g)) * u


def kernel(
    n, tp, cap, chunks,
    x_hbm, gain_hbm, routes_hbm, rw_hbm,
    eg_hbm, eu_hbm, ed_hbm, sg_hbm, su_hbm, sd_hbm,
    out_ref,
    wgu, wd, vg, vu, vd,
    x_ref, gain_ref, routes_ref, rw_ref, xm_ref, meta, metam,
    packed, outbuf, arrive, retbuf, back,
    rows, hid, squares, sssend, ssrecv, shsend, shrecv, acc, shout,
    isem, wsem, dsend, drecv, rsend, rrecv, tsend, trecv, qsend, qrecv, hsend, hrecv, xsend, xrecv, asend, arecv,
    *exchanged,
):
    me = lax.axis_index("ep")
    my_tp = lax.axis_index("tp")
    m, quarter = n // 2, n // 4
    half, inner = me // m, lax.rem(me, m)
    mirror = lax.rem(me + m, n)
    spot = lax.rem(me, quarter)
    bit = lax.rem(me // quarter, 2)
    split_ff = tp == 2
    theirs = 1 - my_tp
    toks, width = x_ref.shape
    picks = routes_ref.shape[0]
    ff = wd.shape[0]
    fs = vg.shape[1]
    blocks = width // LANES
    jc = blocks * cap
    cols = ff // chunks
    mine, psend, precv = exchanged[0::3], exchanged[1::3], exchanged[2::3]

    def mate(i):
        return half * m + lax.rem(inner + i, m)

    def in_quarter(q):
        return [q * quarter + i for i in range(quarter)]

    near = [mate(i) for i in range(m)]
    groups = [near, in_quarter(3 * (1 - half)), in_quarter(2 - half)]
    mirror_group = 1 + lax.rem(bit + 1 - half, 2)
    group_there = 1 + lax.rem(bit + half, 2)

    barrier = pltpu.get_barrier_semaphore()
    pl.semaphore_signal(barrier, inc=1, device_id={"ep": mirror}, device_id_type=MESH)
    for i in range(1, m):
        pl.semaphore_signal(barrier, inc=1, device_id={"ep": mate(i)}, device_id_type=MESH)
    for i in range(1, tp):
        pl.semaphore_signal(barrier, inc=1, device_id={"tp": lax.rem(my_tp + i, tp)}, device_id_type=MESH)

    small = []
    for i, (src, dst) in enumerate(
        ((routes_hbm, routes_ref), (rw_hbm, rw_ref), (x_hbm, x_ref), (gain_hbm, gain_ref))
    ):
        c = pltpu.make_async_copy(src, dst, isem.at[i])
        c.start()
        small.append(c)
    for c in small:
        c.wait()
    loads = {}
    parts = [("sg", sg_hbm, vg), ("su", su_hbm, vu)]
    for c in range(chunks):
        which = (theirs, my_tp)[c] if split_ff else c
        taken = pl.ds(pl.multiple_of(which * cols, LANES), cols)
        parts.append((f"e{c}", eg_hbm.at[0, :, taken], wgu.at[which, :, 0:cols]))
        parts.append((f"e{c}", eu_hbm.at[0, :, taken], wgu.at[which, :, cols : 2 * cols]))
    parts += [("ed", ed_hbm.at[0], wd), ("sd", sd_hbm, vd)]
    for slot, (name, src, dst) in enumerate(parts):
        c = pltpu.make_async_copy(src, dst, wsem.at[slot])
        c.start()
        loads.setdefault(name, []).append(c)

    def loaded(*names):
        for name in names:
            for c in loads[name]:
                c.wait()

    def places(routes, base, number):
        expert = lax.broadcasted_iota(jnp.int32, (number, toks), 0) + base
        hits = [routes[k : k + 1, :] == expert for k in range(picks)]
        named = jnp.zeros((number, toks), F32)
        for hit in hits:
            named = named + jnp.where(hit, 1.0, 0.0)
        row_i = lax.broadcasted_iota(jnp.int32, (toks, toks), 0)
        col_i = lax.broadcasted_iota(jnp.int32, (toks, toks), 1)
        earlier = jnp.where(row_i < col_i, 1.0, 0.0).astype(BF16)
        before = jnp.dot(named.astype(BF16), earlier, preferred_element_type=F32)
        return hits, jnp.where(named > 0.5, before, -1.0)

    def by_slot(place, v):
        return jnp.concatenate([jnp.where(place == s, v, 0.0) for s in range(cap)], axis=0).astype(BF16)

    def pack(value, j, number):
        for s in range(cap):
            packed[pl.ds(j * cap + s, number, stride=jc), :] = value[s * number : (s + 1) * number, :]

    def unpack(j, number):
        return jnp.concatenate(
            [packed[pl.ds(j * cap + s, number, stride=jc), :] for s in range(cap)], axis=0
        )

    def select_rows(g, routes, x):
        select = by_slot(places(routes, half * m, m)[1], 1.0)
        for j in range(blocks):
            cut = slice(j * LANES, (j + 1) * LANES)
            pack(jnp.dot(select, x[:, cut], preferred_element_type=F32), j, m)
        for p in range(m):
            outbuf[g, p] = packed[pl.ds(p * jc, jc), :].astype(BF16)

    pending = []

    def to_tp(src, dst_of, send_of, recv_of):
        copies = []
        for i in range(1, tp):
            c = pltpu.make_async_remote_copy(
                src_ref=src, dst_ref=dst_of(i - 1), send_sem=send_of(i - 1), recv_sem=recv_of(i - 1),
                device_id={"tp": lax.rem(my_tp + i, tp)}, device_id_type=MESH,
            )
            c.start()
            copies.append(c)
        pending.extend(copies)
        return copies

    def to_mirror(src, dst, at):
        c = pltpu.make_async_remote_copy(
            src_ref=src, dst_ref=dst, send_sem=xsend.at[at], recv_sem=xrecv.at[at],
            device_id={"ep": mirror}, device_id_type=MESH,
        )
        c.start()
        pending.append(c)
        return c

    def token_copies(g, home):
        for i in range(1, m):
            to = lax.rem(inner + i, m)
            pltpu.make_async_remote_copy(
                src_ref=outbuf.at[g, to], dst_ref=arrive.at[home], send_sem=dsend.at[g],
                recv_sem=drecv.at[g * mirror_group], device_id={"ep": mate(i)}, device_id_type=MESH,
            ).start()
        arrive[home] = outbuf[g, inner]

    def many(ref, number, send, recv):
        part = ref.at[pl.ds(0, number)]
        return pltpu.make_async_remote_copy(
            src_ref=part, dst_ref=part, send_sem=send, recv_sem=recv,
            device_id={"ep": mirror}, device_id_type=MESH,
        )

    def wait_tokens(g):
        if g == 0:
            many(arrive, m - 1, dsend.at[0], drecv.at[0]).wait_recv()
            return

        @pl.when(mirror_group == g)
        def _():
            many(arrive, quarter - 1, dsend.at[0], drecv.at[g]).wait_recv()

        @pl.when(mirror_group != g)
        def _():
            many(arrive, quarter, dsend.at[0], drecv.at[g]).wait_recv()

    def send_back(g):
        for i, home in enumerate(groups[g]):
            if g or i:
                pltpu.make_async_remote_copy(
                    src_ref=retbuf.at[home], dst_ref=back.at[me], send_sem=rsend.at[g],
                    recv_sem=rrecv.at[group_there if g else 0], device_id={"ep": home}, device_id_type=MESH,
                ).start()

    def returned(g):
        return many(back, quarter if g else m - 1, rsend.at[g], rrecv.at[g])

    routes = routes_ref[...]
    meta[0:picks, 0:toks] = routes.astype(F32)
    x = x_ref[...]
    gain = gain_ref[...]
    select_rows(0, routes, x)
    pl.semaphore_wait(barrier, m + tp - 1)
    mcopy = to_mirror(meta, metam, 1)
    xcopy = to_mirror(x_ref, xm_ref, 0)
    token_copies(0, me)
    rw = rw_ref[...]
    scaled = 2.5 * rw / jnp.sum(rw, axis=0, keepdims=True)

    def combiner(base, number):
        hits, place = places(routes, base, number)
        weight = jnp.zeros((number, toks), F32)
        for k in range(picks):
            weight = weight + jnp.where(hits[k], scaled[k : k + 1, :], 0.0)
        w_hi = weight.astype(BF16).astype(F32)
        return by_slot(place, w_hi), by_slot(place, weight - w_hi)

    bases = half * m, 3 * (1 - half) * quarter, (2 - half) * quarter
    combiners = [combiner(base, len(group)) for base, group in zip(bases, groups)]
    rows[...] = jnp.zeros(rows.shape, BF16)
    xf = x.astype(F32)
    xg = (xf * gain).astype(BF16)
    ss_own = jnp.sum(xf * xf, axis=1, keepdims=True)
    shsend[...] = jnp.zeros(shsend.shape, F32)
    shsend[0:toks, 2 * fs : 2 * fs + LANES] = jnp.broadcast_to(ss_own, (toks, LANES))
    for name, w, base in (("sg", vg, 0), ("su", vu, fs)):
        loaded(name)
        shsend[0:toks, base : base + fs] = jnp.dot(xg, w[...], preferred_element_type=F32)
    shared = to_tp(shsend, lambda i: shrecv.at[i], lambda i: hsend.at[i], lambda i: hrecv.at[i])
    def serve_mirror():
        mcopy.wait_recv()
        xcopy.wait_recv()
        select_rows(1, metam[0:picks, 0:toks].astype(jnp.int32), xm_ref[...])
        token_copies(1, mirror)

    pl.when(me >= quarter)(serve_mirror)

    def finish_shared(copies):
        loaded("sd")
        for c in copies:
            c.wait_recv()
        total = shsend[...]
        for i in range(tp - 1):
            total = total + shrecv[i]
        r_own = lax.rsqrt(total[:, 2 * fs : 2 * fs + 1] / (width * tp) + 1e-06)
        sh_hidden = silu_mul(total[:, 0:fs] * r_own, total[:, fs : 2 * fs] * r_own).astype(BF16)
        shout[...] = jnp.dot(sh_hidden, vd[...], preferred_element_type=F32)

    def first_half(g):
        number = len(groups[g])
        count = number * cap
        low = -(-count // 16) * 16
        wait_tokens(g)
        for i, home in enumerate(groups[g]):
            packed[pl.ds(i * jc, jc), :] = arrive[home].astype(F32)
        ss = jnp.zeros((count, LANES), F32)
        for j in range(blocks):
            cut = slice(j * LANES, (j + 1) * LANES)
            piece = unpack(j, number)
            ss = ss + piece * piece
            scaled_piece = piece * gain[:, cut]
            hi = scaled_piece.astype(BF16)
            rows[0:count, cut] = hi
            rows[low : low + count, cut] = (scaled_piece - hi.astype(F32)).astype(BF16)
        squares[0:count, :] = jnp.broadcast_to(jnp.sum(ss, axis=1, keepdims=True), (count, LANES))
        sssend[g] = squares[...].T[0:8, :]
        all_copies = [to_tp(
            sssend.at[g], lambda i: ssrecv.at[i, g],
            lambda i: qsend.at[i * len(groups) + g], lambda i: qrecv.at[i * len(groups) + g],
        )]
        taken_rows = rows[0 : 2 * low, :]
        for c in range(chunks):
            loaded_once(c)
            own = split_ff and g == 0 and c > 0
            which = (theirs, my_tp)[c] if split_ff else c
            v = jnp.dot(taken_rows, wgu[which], preferred_element_type=F32)
            v = v[0:count] + v[low : low + count]
            mine[g][c] = v
            if own:
                continue
            psend[g][c] = v.astype(BF16)
            at_sem = lambda i: (i * len(groups) + g) * chunks + c
            all_copies.append(to_tp(
                psend[g].at[c], lambda i: precv[g].at[i, c],
                lambda i: tsend.at[at_sem(i)], lambda i: trecv.at[at_sem(i)],
            ))
        return all_copies

    def scale(g, copies):
        for c in copies:
            c.wait_recv()
        ss_all = sssend[g]
        for i in range(tp - 1):
            ss_all = ss_all + ssrecv[i, g]
        r_all = lax.rsqrt(ss_all / (width * tp) + 1e-06)
        return jnp.broadcast_to(r_all[0:1, :], squares.shape[::-1]).T[0 : len(groups[g]) * cap, 0:1]

    def activate(both, r):
        return silu_mul(both[:, 0:cols] * r, both[:, cols : 2 * cols] * r).astype(BF16)

    def deliver(g, value_of):
        number = len(groups[g])
        for j in range(blocks):
            pack(value_of(slice(j * LANES, (j + 1) * LANES)), j, number)
        for i, home in enumerate(groups[g]):
            retbuf[home] = packed[pl.ds(i * jc, jc), :].astype(BF16)
        send_back(g)
        if g == 0:
            back[me] = retbuf[me]

    def hidden_copy():
        return pltpu.make_async_remote_copy(
            src_ref=hid.at[my_tp], dst_ref=hid.at[my_tp], send_sem=asend.at[0], recv_sem=arecv.at[0],
            device_id={"tp": theirs}, device_id_type=MESH,
        )

    def hidden_half(all_copies):
        r = scale(0, all_copies[0])
        for c in all_copies[1]:
            c.wait_recv()
        hid[my_tp] = activate(mine[0][1] + precv[0][0, 0].astype(F32), r)
        hidden_copy().start()

    def out_half():
        hidden_copy().wait_recv()
        acc[0 : m * cap, :] = jnp.dot(hid[0], wd[0:cols, :], preferred_element_type=F32)
        part = jnp.dot(hid[1], wd[cols : 2 * cols, :], preferred_element_type=F32)
        deliver(0, lambda cut: acc[0 : m * cap, cut] + part[:, cut])

    def second_half(g, all_copies):
        count = len(groups[g]) * cap
        r = scale(g, all_copies[0])
        for c in range(chunks):
            for copy in all_copies[1 + c]:
                copy.wait_recv()
            which = (my_tp, theirs)[c] if split_ff else c
            both = mine[g][1 - c if split_ff else c]
            for i in range(tp - 1):
                both = both + precv[g][i, c].astype(F32)
            hidden = activate(both, r)
            part = jnp.dot(hidden, wd[pl.ds(pl.multiple_of(which * cols, LANES), cols), :], preferred_element_type=F32)
            if c == 0:
                acc[0:count, :] = part
            elif c < chunks - 1:
                acc[0:count, :] += part
            else:
                deliver(g, lambda cut: acc[0:count, cut] + part[:, cut])

    fetched = set()

    def loaded_once(c):
        if c not in fetched:
            fetched.add(c)
            loaded(f"e{c}")

    def only(where, step):
        if split_ff:
            pl.when(where)(step)

    lower, upper = half == 0, half == 1
    state0 = first_half(0)
    pl.when(me < quarter)(serve_mirror)
    state1 = first_half(1)
    only(lower, lambda: hidden_half(state0))
    state2 = first_half(2)
    only(upper, lambda: hidden_half(state0))
    loaded("ed")
    if not split_ff:
        second_half(0, state0)
    second_half(1, state1)
    only(lower, out_half)
    second_half(2, state2)
    only(upper, out_half)
    finish_shared(shared)

    def combined(g):
        number = len(groups[g])
        for p in range(number):
            packed[pl.ds(p * jc, jc), :] = back[bases[g] + p].astype(F32)
        for j in range(blocks):
            cut = slice(j * LANES, (j + 1) * LANES)
            piece = unpack(j, number).astype(BF16)
            routed = lax.dot_general(combiners[g][0], piece, TN, preferred_element_type=F32)
            routed = routed + lax.dot_general(combiners[g][1], piece, TN, preferred_element_type=F32)
            yield cut, shout[0:toks, cut] + routed

    for g in (1, 0, 2):
        returned(g).wait_recv()
        for cut, value in combined(g):
            if g < len(groups) - 1:
                shout[0:toks, cut] = value
            else:
                out_ref[:, cut] = value.astype(BF16)
    for c in pending:
        c.wait_send()
    for g in range(2):
        many(arrive, m - 1, dsend.at[g], drecv.at[g]).wait_send()
    for g in range(len(groups)):
        returned(g).wait_send()
    if split_ff:
        hidden_copy().wait_send()


def local(tokens, norm_gain, routes, route_weights, eg, eu, ed, sg, su, sd):
    toks, width = tokens.shape
    picks = routes.shape[1]
    n, tp = lax.axis_size("ep"), lax.axis_size("tp")
    cap = max(2, toks * picks // n + 1)
    ff, fs = eg.shape[2], sg.shape[1]
    chunks = 2
    m, quarter = n // 2, n // 4
    jc = width // LANES * cap
    low = -(-m * cap // 16) * 16
    padded = -(-toks // 16) * 16
    cols = ff // chunks
    others = max(1, tp - 1)
    split = -(-picks // 8) * 8
    sizes = (m, quarter, quarter)
    slots = -(-m * cap // LANES) * LANES
    exchanged = []
    for s in sizes:
        exchanged += [
            pltpu.VMEM((chunks, s * cap, 2 * cols), F32),
            pltpu.VMEM((chunks, s * cap, 2 * cols), BF16),
            pltpu.VMEM((others, chunks, s * cap, 2 * cols), BF16),
        ]
    hbm = pl.BlockSpec(memory_space=pl.ANY)
    dma = pltpu.SemaphoreType.DMA
    return pl.pallas_call(
        functools.partial(kernel, n, tp, cap, chunks),
        out_shape=pltpu.VMEM((toks, width), BF16),
        in_specs=[hbm] * 10,
        out_specs=pl.BlockSpec(memory_space=pltpu.VMEM),
        scratch_shapes=[
            pltpu.VMEM((chunks, width, 2 * cols), BF16), pltpu.VMEM((ff, width), BF16),
            pltpu.VMEM((width, fs), BF16), pltpu.VMEM((width, fs), BF16), pltpu.VMEM((fs, width), BF16),
            pltpu.VMEM((toks, width), BF16), pltpu.VMEM((1, width), F32),
            pltpu.VMEM((picks, toks), jnp.int32), pltpu.VMEM((picks, toks), F32),
            pltpu.VMEM((toks, width), BF16),
            pltpu.VMEM((split, LANES), F32), pltpu.VMEM((split, LANES), F32),
            pltpu.VMEM((n * jc, LANES), F32),
            pltpu.VMEM((2, m, jc, LANES), BF16), pltpu.VMEM((n, jc, LANES), BF16),
            pltpu.VMEM((n, jc, LANES), BF16), pltpu.VMEM((n, jc, LANES), BF16),
            pltpu.VMEM((2 * low, width), BF16), pltpu.VMEM((chunks, m * cap, cols), BF16),
            pltpu.VMEM((slots, LANES), F32),
            pltpu.VMEM((3, 8, slots), F32), pltpu.VMEM((others, 3, 8, slots), F32),
            pltpu.VMEM((padded, 2 * fs + LANES), F32), pltpu.VMEM((others, padded, 2 * fs + LANES), F32),
            pltpu.VMEM((m * cap, width), F32), pltpu.VMEM((padded, width), F32),
            dma((4,)), dma((4 + 2 * chunks,)),
            dma((2,)), dma((3,)), dma((3,)), dma((3,)),
            dma((others * chunks * 3,)), dma((others * chunks * 3,)),
            dma((others * 3,)), dma((others * 3,)), dma((others,)), dma((others,)), dma((2,)), dma((2,)),
            dma((1,)), dma((1,)),
        ] + exchanged,
        compiler_params=pltpu.CompilerParams(
            collective_id=0, has_side_effects=True, vmem_limit_bytes=60 * 1024 * 1024
        ),
    )(tokens, norm_gain.reshape(1, width), routes.T, route_weights.T, eg, eu, ed, sg, su, sd)


def solution(mesh):
    placed = (
        P("ep", "tp"),
        P("tp"),
        P("ep", None),
        P("ep", None),
        P("ep", "tp", None),
        P("ep", "tp", None),
        P("ep", None, "tp"),
        P("tp", None),
        P("tp", None),
        P(None, "tp"),
    )
    return jax.shard_map(
        local, mesh=mesh, in_specs=placed, out_specs=P("ep", "tp"), check_vma=False
    )
```
